128 devices in a mesh: sp: 32 (over z, y, core), tp: 4 (over x).
Axes of the slice: x: 4, y: 4, z: 4, core: 2. Of those that a mesh axis runs over, the one named last changes fastest.
Arguments:
- query_narrow: bfloat16 [4096, 2048], P('sp', 'tp'), may hold values from -48 to 48
- key_narrow: bfloat16 [4096, 512], P('sp', 'tp'), may hold values from -15 to 15
- value_narrow: bfloat16 [4096, 512], P('sp', 'tp'), may hold values from -6 to 6
- gates_narrow: float32 [4096, 16], P(None, 'tp'), may hold values from -514 to 0, as said below
- query_broad: bfloat16 [4096, 2048], P('sp', 'tp'), may hold values from -48 to 48
- key_broad: bfloat16 [4096, 1024], P('sp', 'tp'), may hold values from -15 to 15
- value_broad: bfloat16 [4096, 1024], P('sp', 'tp'), may hold values from -6 to 6
- gates_broad: float32 [4096, 8], P(None, 'tp'), may hold values from -514 to 0, as said below
- project_narrow: bfloat16 [2048, 4096], P('tp'), may hold values from -0.1875 to 0.1875
- project_broad: bfloat16 [2048, 4096], P('tp'), may hold values from -0.1875 to 0.1875
- residual: bfloat16 [4096, 4096], P('sp'), may hold values from -6 to 6
- norm_gain: float32 [4096], replicated, may hold values from 0.1 to 1.9
- route_ids: int32 [4096, 4], P(('sp', 'tp')), may hold values from 0 to 127, all different within a row; in each aligned block of 32 rows (0 to 31, 32 to 63, ...) at most 2 rows name the same one
- route_weight: float32 [4096, 4], P(('sp', 'tp')), may hold values from 0.2 to 1.2
- expert_gate: bfloat16 [128, 4096, 256], P(('sp', 'tp')), may hold values from -0.09375 to 0.09375
- expert_up: bfloat16 [128, 4096, 256], P(('sp', 'tp')), may hold values from -0.09375 to 0.09375
- expert_down: bfloat16 [128, 256, 4096], P(('sp', 'tp')), may hold values from -0.375 to 0.375
- shared_gate: bfloat16 [4096, 1024], P(None, 'tp'), may hold values from -0.09375 to 0.09375
- shared_up: bfloat16 [4096, 1024], P(None, 'tp'), may hold values from -0.09375 to 0.09375
- shared_down: bfloat16 [1024, 4096], P('tp'), may hold values from -0.1875 to 0.1875
Outputs:
- layer_out: bfloat16 [4096, 4096], P(('sp', 'tp'))
The draws below stay inside these ranges and needn't reach their ends.
Inputs may be any that keep to these rules, and one draw needn't show every extreme that they name: `gates_narrow`: Non-increasing along positions in each head. `gates_broad`: Non-increasing along positions in each head. `route_ids`: each row names 4 different experts; among the rows of one device no expert is named by more than 2 rows, and that number is reached.
All inputs are finite; a program needn't handle non-finite values.
Results may differ from the reference program's by a relative error of at most 0.014.
Values may be sent and summed in bfloat16 or wider, within the bound.
A program may use at most 128 MiB of HBM per device.

```python
import math
import jax
import jax.numpy as jnp
import numpy as np
from jax import lax

D = 4096
NARROW_HEADS = 16
NARROW_SIZE = 128
NARROW_KV = 4
BROAD_HEADS = 8
BROAD_SIZE = 256
BROAD_KV = 4
EXPERT_WIDTH = 256
SHARED_WIDTH = 1024
TOP = 4
TOK_DEV = 128
SEQUENCE_LENGTH = 4096
TOK_SUB = 32
EXPERTS = 128
CAP = 2
ATT_W = 4096
N_SP = 32
N_TP = 4


def plant_pairs(key, head_count, kv_heads, head_size, salt):
    base = jax.random.fold_in(key, salt)
    sequence_lanes = jax.random.split(base, 7)
    key_rows = 2.5 * jnp.clip(jax.random.normal(sequence_lanes[5], (SEQUENCE_LENGTH, kv_heads * head_size), jnp.float32), -6.0, 6.0)
    query_rows = jnp.clip(jax.random.normal(sequence_lanes[6], (SEQUENCE_LENGTH, head_count * head_size), jnp.float32), -6.0, 6.0)
    return (query_rows, key_rows)


def forget_cumulative(key, head_count, salt):
    base = jax.random.fold_in(key, salt)
    sequence_lanes = jax.random.split(base, 5)
    rough = jnp.exp(jax.random.uniform(sequence_lanes[0], (SEQUENCE_LENGTH, head_count), jnp.float32, math.log(0.5), math.log(2.0)))
    block_rate = jnp.exp(jax.random.uniform(sequence_lanes[1], (SEQUENCE_LENGTH // TOK_DEV, head_count), jnp.float32, math.log(0.5), math.log(2.0)))
    block_rate = jnp.repeat(block_rate, TOK_DEV, axis=0)
    order = jax.random.permutation(sequence_lanes[2], head_count)
    quick = order < head_count // 2
    rate = jnp.where(quick, 1.0 / 40.0, 0.4 / SEQUENCE_LENGTH)
    gate_logarithm = -rate[None, :] * rough * block_rate
    segment_start = jax.random.randint(sequence_lanes[3], (2, head_count), 0, SEQUENCE_LENGTH)
    segment_length = jax.random.uniform(sequence_lanes[4], (2, head_count), jnp.float32, math.log(0.5), math.log(0.8))
    place_indices = jnp.arange(SEQUENCE_LENGTH, dtype=jnp.int32)[:, None]
    for round_index in range(2):
        gate_logarithm = gate_logarithm + jnp.where(place_indices == segment_start[round_index][None, :], segment_length[round_index][None, :], 0.0)
    return jnp.cumsum(gate_logarithm, axis=0)


def draw_query_narrow(key, part):
    return plant_pairs(key, NARROW_HEADS, NARROW_KV, NARROW_SIZE, 101)[0].astype(jnp.bfloat16)


def draw_key_narrow(key, part):
    return plant_pairs(key, NARROW_HEADS, NARROW_KV, NARROW_SIZE, 101)[1].astype(jnp.bfloat16)


def draw_query_broad(key, part):
    return plant_pairs(key, BROAD_HEADS, BROAD_KV, BROAD_SIZE, 202)[0].astype(jnp.bfloat16)


def draw_key_broad(key, part):
    return plant_pairs(key, BROAD_HEADS, BROAD_KV, BROAD_SIZE, 202)[1].astype(jnp.bfloat16)


def draw_gates_narrow(key, part):
    return forget_cumulative(key, NARROW_HEADS, 303)


def draw_gates_broad(key, part):
    return forget_cumulative(key, BROAD_HEADS, 404)


def block_scale(own_key, shape, shards, smallest, top_value):
    def one(dim, blocks):
        steps = jax.random.uniform(jax.random.fold_in(jax.random.fold_in(own_key, 6), dim), (blocks,), jnp.float32, smallest / len(shards), top_value / len(shards))
        return jnp.repeat(jnp.exp(steps), shape[dim] // blocks).reshape((-1,) + (1,) * (len(shape) - dim - 1))

    gain = one(*shards[0])
    for cut in shards[1:]:
        gain = gain * one(*cut)
    return gain


def shared_out(stream_key, own, number, rows, count, top, reach, slope):
    ranking = jax.random.permutation(stream_key, count)
    packed, usual = shares(count, rows * top, reach, slope, True), shares(count, rows * top, reach, slope, False)
    places = jnp.arange(count)

    def named(tallies, turn):
        used = int((tallies > 0).sum())
        fixed = max(1, used // 4)
        moved = fixed + (places - fixed + turn * (used - fixed)) % max(1, count - fixed)
        return jnp.zeros((count,), jnp.int32).at[ranking[jnp.where(places < fixed, places, moved)]].set(jnp.asarray(tallies, jnp.int32))

    tallies = jnp.where(number % 4 == 0, named(packed, number // 4), named(usual, number - number // 4 - 1))
    mixed = jax.random.permutation(jax.random.fold_in(own, 3), count)
    donor, sink = mixed[0:count // 2 * 2:2], mixed[1:count // 2 * 2:2]
    slack = jnp.minimum(tallies[donor] - 1, reach - tallies[sink]) // 2
    slack = jnp.where((donor == ranking[0]) | (sink == ranking[0]) | (tallies[sink] == 0), 0, jnp.maximum(slack, 0))
    moved = jax.random.randint(jax.random.fold_in(own, 4), (count // 2,), 0, 1 << 20) % (slack + 1)
    tallies = tallies.at[donor].add(-moved).at[sink].add(moved)
    items = jnp.searchsorted(jnp.cumsum(tallies), jnp.arange(rows * top), side="right").astype(jnp.int32)
    grid = items.reshape(top, rows).T
    grid = grid[jax.random.permutation(jax.random.fold_in(own, 1), rows)]
    turn = jax.random.randint(jax.random.fold_in(own, 2), (rows, 1), 0, top)
    return jnp.take_along_axis(grid, (jnp.arange(top)[None, :] + turn) % top, axis=1)


def shares(amount, total, bound, skew, full):
    portions = [(1 << 20) // math.isqrt(rank ** skew) + 1 for rank in range(1, amount + 1)]
    largest = bound if full else min(bound, max(-(-total // amount), total * portions[0] // sum(portions)))
    least = 1 if total - largest >= amount - 1 else 0
    holding, surplus = [largest] + [least] * (amount - 1), total - largest - least * (amount - 1)
    while surplus > 0:
        movable = [i for i in range(1, amount) if holding[i] < largest] or [i for i in range(1, amount) if holding[i] < bound]
        pool, left = sum([portions[i] for i in movable]), surplus
        for i in movable:
            more = min(bound - holding[i], max(1, left * portions[i] // pool), surplus)
            holding[i] = holding[i] + more
            surplus = surplus - more
    return np.array(holding)


def centred(stream_key, shape, deviation, most, shards=(), held_as=jnp.bfloat16):
    gain = block_scale(stream_key, shape, shards, -0.22, 0.18) if shards else 1.0
    values = jax.random.normal(stream_key, shape, jnp.float32) * deviation * gain
    return jnp.minimum(jnp.maximum(values, -most), most).astype(held_as)


def setup_inputs(seed: int = 0) -> dict:
    key_list = jax.random.split(jax.random.key(seed), 21)
    query_narrow = draw_query_narrow(jax.random.fold_in(key_list[20], 71), 0)
    key_narrow = draw_key_narrow(jax.random.fold_in(key_list[20], 71), 0)
    value_narrow = centred(key_list[2], (SEQUENCE_LENGTH, NARROW_KV * NARROW_SIZE), 1.0, 6.0, ((0, 32), (1, 4)))
    gates_narrow = draw_gates_narrow(jax.random.fold_in(key_list[20], 71), 0)
    query_broad = draw_query_broad(jax.random.fold_in(key_list[20], 71), 0)
    key_broad = draw_key_broad(jax.random.fold_in(key_list[20], 71), 0)
    value_broad = centred(key_list[6], (SEQUENCE_LENGTH, BROAD_KV * BROAD_SIZE), 1.0, 6.0, ((0, 32), (1, 4)))
    gates_broad = draw_gates_broad(jax.random.fold_in(key_list[20], 71), 0)
    project_narrow = centred(key_list[8], (NARROW_HEADS * NARROW_SIZE, D), (ATT_W // 4) ** -0.5, 0.1875, ((0, 4),))
    project_broad = centred(key_list[9], (BROAD_HEADS * BROAD_SIZE, D), (ATT_W // 4) ** -0.5, 0.1875, ((0, 4),))
    residual = centred(key_list[10], (SEQUENCE_LENGTH, D), 1.0, 6.0, ((0, 32),))
    norm_gain = jnp.clip(1.0 + 0.18 * jax.random.normal(key_list[11], (D,), jnp.float32), 0.1, 1.9)
    route_ids_keys = jax.random.split(jax.random.fold_in(key_list[12], 1), SEQUENCE_LENGTH // TOK_SUB)
    route_ids_turns = jax.random.permutation(jax.random.fold_in(key_list[12], 3), SEQUENCE_LENGTH // TOK_SUB)
    route_ids = jax.vmap(lambda own, number: shared_out(jax.random.fold_in(key_list[12], 2), own, number, TOK_SUB, EXPERTS, TOP, CAP, 1))(route_ids_keys, route_ids_turns).reshape((SEQUENCE_LENGTH, TOP))
    route_weight = jnp.clip(jnp.exp(math.log(1.2) - 1.7917595 * jax.random.uniform(key_list[13], (SEQUENCE_LENGTH, TOP), jnp.float32) ** block_scale(key_list[13], (SEQUENCE_LENGTH, TOP), ((0, 128),), -0.2, 0.2)), 0.2, 1.2)
    expert_gate = centred(key_list[14], (EXPERTS, D, EXPERT_WIDTH), D ** -0.5, 0.09375, ((0, 128),))
    expert_up = centred(key_list[15], (EXPERTS, D, EXPERT_WIDTH), D ** -0.5, 0.09375, ((0, 128),))
    expert_down = centred(key_list[16], (EXPERTS, EXPERT_WIDTH, D), EXPERT_WIDTH ** -0.5, 0.375, ((0, 128),))
    shared_gate = centred(key_list[17], (D, SHARED_WIDTH), D ** -0.5, 0.09375, ((1, 4),))
    shared_up = centred(key_list[18], (D, SHARED_WIDTH), D ** -0.5, 0.09375, ((1, 4),))
    shared_down = centred(key_list[19], (SHARED_WIDTH, D), SHARED_WIDTH ** -0.5, 0.1875, ((0, 4),))
    return {"query_narrow": query_narrow, "key_narrow": key_narrow, "value_narrow": value_narrow, "gates_narrow": gates_narrow, "query_broad": query_broad, "key_broad": key_broad, "value_broad": value_broad, "gates_broad": gates_broad, "project_narrow": project_narrow, "project_broad": project_broad, "residual": residual, "norm_gain": norm_gain, "route_ids": route_ids, "route_weight": route_weight, "expert_gate": expert_gate, "expert_up": expert_up, "expert_down": expert_down, "shared_gate": shared_gate, "shared_up": shared_up, "shared_down": shared_down}


norm_epsilon = 1e-06

def group_attention(queries, key_rows, value_rows, gate_totals, head_count, kv_heads, head_size):
    group_size = head_count // kv_heads
    query_block = 256
    scaling = head_size ** (-0.5)
    outputs = []
    for first_query in range(0, SEQUENCE_LENGTH, query_block):
        last_key = first_query + query_block
        query_heads = queries[first_query:last_key].astype(jnp.float32).reshape(query_block, kv_heads, group_size, head_size)
        key_heads = key_rows[:last_key].astype(jnp.float32).reshape(last_key, kv_heads, head_size)
        value_heads = value_rows[:last_key].astype(jnp.float32).reshape(last_key, kv_heads, head_size)
        scores = jnp.einsum('tkgd,skd->kgts', query_heads, key_heads) * scaling
        query_gates = gate_totals[first_query:last_key].reshape(query_block, kv_heads, group_size).transpose(1, 2, 0)
        key_gates = gate_totals[:last_key].T.reshape(kv_heads, group_size, 1, last_key)
        scores = scores + query_gates[..., None] - key_gates
        allowed = jnp.arange(last_key)[None, :] <= (first_query + jnp.arange(query_block))[:, None]
        scores = jnp.where(allowed, scores, -jnp.inf)
        highest = lax.optimization_barrier(jnp.max(scores, axis=-1, keepdims=True))
        weights = jnp.exp(scores - highest)
        totals = lax.optimization_barrier(jnp.sum(weights, axis=-1))
        rounded = lax.optimization_barrier(weights.astype(jnp.bfloat16)).astype(jnp.float32)
        blended = jnp.einsum('kgts,skd->tkgd', rounded, value_heads) / totals.transpose(2, 0, 1)[..., None]
        outputs.append(blended.reshape(query_block, head_count * head_size).astype(jnp.bfloat16))
    return jnp.concatenate(outputs, axis=0)

def routed_experts(normed, route_ids, route_weight, expert_gate, expert_up, expert_down):
    top_count = route_ids.shape[1]
    flat_ids = route_ids.reshape(-1)
    flat_weight = lax.optimization_barrier(route_weight.reshape(-1).astype(jnp.bfloat16)).astype(jnp.float32)
    most_rows = N_SP * N_TP * CAP

    def one_expert(carried, expert):
        chosen = flat_ids == expert
        picked = jnp.nonzero(chosen, size=most_rows, fill_value=0)[0].astype(jnp.int32)
        live = jnp.arange(most_rows) < jnp.sum(chosen.astype(jnp.int32))
        token_index = picked // top_count
        rows = normed[token_index]
        gate_out = jnp.dot(rows, expert_gate[expert], preferred_element_type=jnp.float32)
        up_out = jnp.dot(rows, expert_up[expert], preferred_element_type=jnp.float32)
        hidden = (jax.nn.silu(gate_out) * up_out).astype(jnp.bfloat16)
        output = jnp.dot(hidden, expert_down[expert], preferred_element_type=jnp.float32)
        output = lax.optimization_barrier(output.astype(jnp.bfloat16)).astype(jnp.float32)
        contribution = jnp.where(live[:, None], flat_weight[picked][:, None] * output, jnp.zeros((), jnp.float32))
        return (carried.at[token_index].add(contribution), None)
    routed, ignored = lax.scan(one_expert, jnp.zeros((SEQUENCE_LENGTH, D), jnp.float32), jnp.arange(EXPERTS, dtype=jnp.int32))
    return routed

def reference(query_narrow, key_narrow, value_narrow, gates_narrow, query_broad, key_broad, value_broad, gates_broad, project_narrow, project_broad, residual, norm_gain, route_ids, route_weight, expert_gate, expert_up, expert_down, shared_gate, shared_up, shared_down):
    narrow = group_attention(query_narrow, key_narrow, value_narrow, gates_narrow, NARROW_HEADS, NARROW_KV, NARROW_SIZE)
    broad = group_attention(query_broad, key_broad, value_broad, gates_broad, BROAD_HEADS, BROAD_KV, BROAD_SIZE)
    width_narrow = NARROW_HEADS * NARROW_SIZE // N_TP
    width_broad = BROAD_HEADS * BROAD_SIZE // N_TP
    mixture = jnp.zeros((SEQUENCE_LENGTH, D), jnp.float32)
    for member in range(N_TP):
        low_n, high_n = (member * width_narrow, (member + 1) * width_narrow)
        low_b, high_b = (member * width_broad, (member + 1) * width_broad)
        portion = jnp.dot(narrow[:, low_n:high_n], project_narrow[low_n:high_n], preferred_element_type=jnp.float32)
        portion = portion + jnp.dot(broad[:, low_b:high_b], project_broad[low_b:high_b], preferred_element_type=jnp.float32)
        mixture = mixture + lax.optimization_barrier(portion.astype(jnp.bfloat16)).astype(jnp.float32)
    stream = residual.astype(jnp.float32) + mixture
    normed = (stream * lax.rsqrt(lax.optimization_barrier(jnp.mean(stream * stream, axis=-1, keepdims=True)) + norm_epsilon) * norm_gain).astype(jnp.bfloat16)
    shared_hidden = (jax.nn.silu(jnp.dot(normed, shared_gate, preferred_element_type=jnp.float32)) * jnp.dot(normed, shared_up, preferred_element_type=jnp.float32)).astype(jnp.bfloat16)
    width_shared = SHARED_WIDTH // N_TP
    shared = jnp.zeros((SEQUENCE_LENGTH, D), jnp.float32)
    for member in range(N_TP):
        low_s, high_s = (member * width_shared, (member + 1) * width_shared)
        portion = jnp.dot(shared_hidden[:, low_s:high_s], shared_down[low_s:high_s], preferred_element_type=jnp.float32)
        shared = shared + lax.optimization_barrier(portion.astype(jnp.bfloat16)).astype(jnp.float32)
    routed = routed_experts(normed, route_ids, route_weight, expert_gate, expert_up, expert_down)
    return (stream + shared + routed).astype(jnp.bfloat16)
```

```python
import math

import jax
import jax.numpy as jnp
from jax import lax
from jax.experimental import pallas as pl
from jax.experimental.pallas import tpu as pltpu
from jax.sharding import PartitionSpec as P

norm_epsilon = 1e-06


MESH = pl.DeviceIdType.MESH
LOG2E = math.log2(math.e)


def flash_heads(q_ref, kv, gate_rows, m_ref, l_ref, acc_ref, heads, size, diagonal):
    keys = kv[:, :size]
    values = kv[:, size:]
    rows = q_ref.shape[0] * q_ref.shape[1]
    length = keys.shape[0]
    scale = size ** (-0.5) * LOG2E
    for h in range(heads):
        q = q_ref[:, :, h * size : (h + 1) * size].reshape(rows, size)
        s = lax.dot_general(q, keys, (((1,), (1,)), ((), ())), preferred_element_type=jnp.float32)
        s = s * scale - gate_rows[h : h + 1, :]
        if diagonal:
            at = lax.broadcasted_iota(jnp.int32, (rows, length), 0)
            to = lax.broadcasted_iota(jnp.int32, (rows, length), 1)
            s = jnp.where(to <= at, s, -jnp.inf)
        top = jnp.broadcast_to(jnp.max(s, axis=1, keepdims=True), (rows, 128))
        if not diagonal:
            before = m_ref[h]
            top = jnp.maximum(before, top)
        p = jnp.exp2(s - jnp.concatenate([top] * (length // 128), axis=1))
        total = jnp.broadcast_to(jnp.sum(p, axis=1, keepdims=True), (rows, 128))
        out = jnp.dot(p.astype(jnp.bfloat16), values, preferred_element_type=jnp.float32)
        if not diagonal:
            factor = jnp.exp2(before - top)
            total = total + l_ref[h] * factor
            out = out + acc_ref[h] * jnp.concatenate([factor] * (size // 128), axis=1)
        m_ref[h] = top
        l_ref[h] = total
        acc_ref[h] = out


def attend_kernel(
    qn_in, kn_in, vn_in, gn_in, qb_in, kb_in, vb_in, gb_in, pn_in, pb_in, res_in, gain_in,
    stream_out, normed_out,
    nkv, bkv, qn, qb, attn, held, mn, ln, accn, mb, lb, accb, wn, wb, res, part, got,
    own_sem, load_sem, own_send, n1_send, n1_recv, b1_send, b1_recv, n2_send, n2_recv, b2_send,
    b2_recv, q_recv, swap_send, swap_recv, r_send, r_recv, a_send, a_recv,
):
    sp = lax.axis_index("sp")
    tp = lax.axis_index("tp")
    z = sp // 8
    y = (sp // 2) % 4
    c = sp % 2
    half = pl.ds(pl.multiple_of(c * 128, 128), 128)

    def at(zz, yy, cc):
        return (zz * 8 + yy * 2 + cc, tp)

    barrier = pltpu.get_barrier_semaphore()
    for step in range(1, 4):
        for cc in range(2):
            pl.semaphore_signal(barrier, inc=1, device_id=at(lax.rem(z + step, 4), y, cc), device_id_type=MESH)
            pl.semaphore_signal(barrier, inc=1, device_id=at(z, lax.rem(y + step, 4), cc), device_id_type=MESH)
        pl.semaphore_signal(barrier, inc=1, device_id=(sp, lax.rem(tp + step, 4)), device_id_type=MESH)
    pl.semaphore_signal(barrier, inc=1, device_id=at(z, y, 1 - c), device_id_type=MESH)

    weights = [
        pltpu.make_async_copy(pn_in, wn, load_sem.at[0]),
        pltpu.make_async_copy(pb_in, wb, load_sem.at[1]),
        pltpu.make_async_copy(res_in.at[pl.ds(pl.multiple_of(tp * 32, 32), 32)], res, load_sem.at[2]),
    ]
    for w in weights:
        w.start()
    pl.semaphore_wait(barrier, 16)

    def remote(src, dst, send, recv, to):
        return pltpu.make_async_remote_copy(
            src_ref=src, dst_ref=dst, send_sem=send, recv_sem=recv, device_id=to, device_id_type=MESH
        )

    nslot = ((kn_in, pl.ds(0, 128)), (vn_in, pl.ds(128, 128)))
    bslot = ((kb_in, pl.ds(0, 256)), (vb_in, pl.ds(256, 256)))

    def n_own(i):
        return nslot[i][0], nkv.at[z, y, half, nslot[i][1]]

    def b_own(i):
        return bslot[i][0], bkv.at[z, y, half, bslot[i][1]]

    n_pairs = [(lambda i=i: n_own(i)) for i in range(2)] + [lambda: (qn_in, qn.at[c])]
    b_pairs = [(lambda i=i: b_own(i)) for i in range(2)] + [lambda: (qb_in, qb.at[c])]

    for role, own, other in ((0, n_pairs, b_pairs), (1, b_pairs, n_pairs)):

        @pl.when(c == role)
        def _(own=own, other=other, role=role):
            for i in range(3):
                src, dst = other[i]()
                remote(src, dst, own_send.at[i], q_recv.at[i], at(z, y, 1 - role)).start()
            for i in range(3):
                src, dst = own[i]()
                pltpu.make_async_copy(src, dst, own_sem.at[i]).start()

    for step in range(1, 4):

        @pl.when(z + step < 4)
        def _(step=step):
            for i in range(2):
                src, dst = n_own(i)
                remote(src, dst, n1_send.at[step, i], n1_recv.at[z, c, i], at(z + step, y, 0)).start()

        for i in range(2):
            src, dst = b_own(i)
            remote(
                src, dst, b1_send.at[step, i], b1_recv.at[y, c, i], at(z, lax.rem(y + step, 4), 1)
            ).start()

    def own_wait(role, own, other):
        for i in range(3):
            src, dst = own[i]()
            pltpu.make_async_copy(src, dst, own_sem.at[i]).wait()
        oc = 1 - role
        ohalf = pl.ds(oc * 128, 128)
        if role == 0:
            dsts = [nkv.at[z, y, ohalf, nslot[i][1]] for i in range(2)] + [qn.at[oc]]
            srcs = [kn_in, vn_in, qn_in]
        else:
            dsts = [bkv.at[z, y, ohalf, bslot[i][1]] for i in range(2)] + [qb.at[oc]]
            srcs = [kb_in, vb_in, qb_in]
        for i in range(3):
            remote(srcs[i], dsts[i], own_send.at[i], q_recv.at[i], at(z, y, oc)).wait_recv()

    @pl.when(c == 0)
    def _():
        own_wait(0, n_pairs, b_pairs)

        def n2(zz, step, yy=None):
            to = y + step if yy is None else yy
            return remote(
                nkv.at[zz, y], nkv.at[zz, y], n2_send.at[zz, step], n2_recv.at[zz, y],
                at(z, lax.rem(y + step, 4), 0),
            )

        def send_on(zz):
            for step in range(1, 4):
                @pl.when((zz < z) | (y + step < 4))
                def _(step=step):
                    n2(zz, step).start()

        def block(zz, yy, diagonal):
            flash_heads(
                qn, nkv[zz, yy], gn_in[zz * 4 + yy], mn, ln, accn, 4, 128, diagonal
            )

        send_on(z)
        block(z, y, True)

        def column(t, carry):
            zz = z - t
            for cc in range(2):
                for i in range(2):
                    remote(
                        nslot[i][0], nkv.at[zz, y, pl.ds(cc * 128, 128), nslot[i][1]],
                        n1_send.at[1, i], n1_recv.at[zz, cc, i], at(zz, y, 0),
                    ).wait_recv()
            send_on(zz)
            block(zz, y, False)
            return carry

        lax.fori_loop(1, z + 1, column, 0)

        def rest(t, carry):
            zz = z - t // 3
            yy = lax.rem(y + t % 3 + 1, 4)

            @pl.when((zz < z) | (yy < y))
            def _():
                remote(
                    nkv.at[zz, yy], nkv.at[zz, yy], n2_send.at[zz, 1], n2_recv.at[zz, yy],
                    at(z, yy, 0),
                ).wait_recv()
                block(zz, yy, False)

            return carry

        lax.fori_loop(0, 3 * (z + 1), rest, 0)
        for h in range(4):
            out = (accn[h] / ln[h]).astype(jnp.bfloat16)
            held[:, :, h * 128 : (h + 1) * 128] = out.reshape(2, 128, 128)
        remote(
            held.at[1], attn.at[0], swap_send, swap_recv, at(z, y, 1)
        ).start()
        attn[0] = held[0]

        def drain(t, carry):
            for step in range(1, 4):
                @pl.when((t < z) | (y + step < 4))
                def _(step=step):
                    n2(t, step).wait_send()
            return carry

        lax.fori_loop(0, z + 1, drain, 0)

    @pl.when(c == 1)
    def _():
        own_wait(1, b_pairs, n_pairs)

        def b2(yy, step):
            return remote(
                bkv.at[z, yy], bkv.at[z, yy], b2_send.at[yy, step], b2_recv.at[z, yy],
                at(z + step, y, 1),
            )

        def send_on(yy):
            for step in range(1, 4):
                @pl.when(z + step < 4)
                def _(step=step):
                    b2(yy, step).start()

        def block(zz, yy, diagonal):
            flash_heads(qb, bkv[zz, yy], gb_in[zz * 4 + yy], mb, lb, accb, 2, 256, diagonal)

        send_on(y)
        block(z, y, True)

        def row(t, carry):
            yy = lax.rem(y + t, 4)
            for cc in range(2):
                for i in range(2):
                    remote(
                        bslot[i][0], bkv.at[z, yy, pl.ds(cc * 128, 128), bslot[i][1]],
                        b1_send.at[1, i], b1_recv.at[yy, cc, i], at(z, yy, 1),
                    ).wait_recv()
            send_on(yy)

            @pl.when(yy < y)
            def _():
                block(z, yy, False)

            return carry

        lax.fori_loop(1, 4, row, 0)

        def rest(t, carry):
            zz = z - 1 - t // 4
            yy = lax.rem(y + t, 4)
            remote(
                bkv.at[zz, yy], bkv.at[zz, yy], b2_send.at[yy, 1], b2_recv.at[zz, yy], at(zz, y, 1)
            ).wait_recv()
            block(zz, yy, False)
            return carry

        lax.fori_loop(0, 4 * z, rest, 0)
        for h in range(2):
            out = (accb[h] / jnp.concatenate([lb[h]] * 2, axis=1)).astype(jnp.bfloat16)
            held[:, :, h * 256 : (h + 1) * 256] = out.reshape(2, 128, 256)
        remote(
            held.at[0], attn.at[1], swap_send, swap_recv, at(z, y, 0)
        ).start()
        attn[1] = held[1]

        def drain(t, carry):
            for step in range(1, 4):
                @pl.when(z + step < 4)
                def _(step=step):
                    b2(t, step).wait_send()
            return carry

        lax.fori_loop(0, 4, drain, 0)

    for i in range(3):
        src, dst = n_pairs[i]() if i < 2 else n_pairs[2]()

        @pl.when(c == 1)
        def _(i=i):
            src, dst = n_pairs[i]()
            remote(src, dst, own_send.at[i], q_recv.at[i], at(z, y, 0)).wait_send()

        @pl.when(c == 0)
        def _(i=i):
            src, dst = b_pairs[i]()
            remote(src, dst, own_send.at[i], q_recv.at[i], at(z, y, 1)).wait_send()

    for step in range(1, 4):

        @pl.when(z + step < 4)
        def _(step=step):
            for i in range(2):
                src, dst = n_own(i)
                remote(src, dst, n1_send.at[step, i], n1_recv.at[z, c, i], at(z + step, y, 0)).wait_send()

        for i in range(2):
            src, dst = b_own(i)
            remote(
                src, dst, b1_send.at[step, i], b1_recv.at[y, c, i], at(z, lax.rem(y + step, 4), 1)
            ).wait_send()

    remote(held.at[1 - c], attn.at[1 - c], swap_send, swap_recv, at(z, y, 1 - c)).wait()
    for w in weights:
        w.wait()

    CH = 1024
    NC = 4096 // CH

    def sent(n, step):
        to = lax.rem(tp + step, 4)
        return remote(
            part.at[n, to], got.at[n, tp], r_send.at[n, step], r_recv.at[n, tp], (sp, to)
        )

    for n in range(NC):
        cols = pl.ds(n * CH, CH)
        p = jnp.dot(attn[0], wn[:, cols], preferred_element_type=jnp.float32)
        p = p + jnp.dot(attn[1], wb[:, cols], preferred_element_type=jnp.float32)
        part[n] = p.astype(jnp.bfloat16).reshape(4, 32, CH)
        for step in range(1, 4):
            sent(n, step).start()

    squares = jnp.zeros((32, 128), jnp.float32)
    for n in range(NC):
        for step in range(1, 4):
            frm = lax.rem(tp + step, 4)
            remote(
                part.at[n, frm], got.at[n, frm], r_send.at[n, step], r_recv.at[n, frm], (sp, frm)
            ).wait_recv()
        cols = pl.ds(n * CH, CH)
        total = res[:, cols].astype(jnp.float32) + part[n, tp].astype(jnp.float32)
        for step in range(1, 4):
            total = total + got[n, lax.rem(tp + step, 4)].astype(jnp.float32)
        stream_out[:, cols] = total
        sq = total * total
        for k in range(CH // 128):
            squares = squares + sq[:, k * 128 : (k + 1) * 128]
    mean = jnp.sum(squares, axis=1, keepdims=True) * (1.0 / 4096)
    rate = lax.rsqrt(mean + norm_epsilon)
    mine = pl.ds(pl.multiple_of(tp * 32, 32), 32)
    for n in range(NC):
        cols = pl.ds(n * CH, CH)
        normed_out[mine, cols] = (stream_out[:, cols] * rate * gain_in[:, cols]).astype(jnp.bfloat16)
    for step in range(1, 4):
        to = lax.rem(tp + step, 4)
        remote(
            normed_out.at[mine], normed_out.at[mine], a_send.at[step], a_recv.at[tp], (sp, to)
        ).start()
    for step in range(1, 4):
        frm = lax.rem(tp + step, 4)
        theirs = pl.ds(pl.multiple_of(frm * 32, 32), 32)
        remote(
            normed_out.at[theirs], normed_out.at[theirs], a_send.at[step], a_recv.at[frm], (sp, frm)
        ).wait_recv()
    for step in range(1, 4):
        to = lax.rem(tp + step, 4)
        remote(
            normed_out.at[mine], normed_out.at[mine], a_send.at[step], a_recv.at[tp], (sp, to)
        ).wait_send()
    for n in range(NC):
        for step in range(1, 4):
            sent(n, step).wait_send()


def attend(qn, kn, vn, gn, qb, kb, vb, gb, pn, pb, residual, gain):
    any_ = pl.BlockSpec(memory_space=pl.ANY)
    vm = pl.BlockSpec(memory_space=pltpu.VMEM)
    dma = pltpu.SemaphoreType.DMA
    f32, b16 = jnp.float32, jnp.bfloat16

    def rows(g):
        return (g * LOG2E).T.reshape(g.shape[1], 16, 256).transpose(1, 0, 2)

    return pl.pallas_call(
        attend_kernel,
        out_shape=(
            jax.ShapeDtypeStruct((32, 4096), f32),
            jax.ShapeDtypeStruct((128, 4096), b16),
        ),
        in_specs=[any_, any_, any_, vm, any_, any_, any_, vm, any_, any_, any_, vm],
        out_specs=(vm, vm),
        scratch_shapes=[
            pltpu.VMEM((4, 4, 256, 256), b16),
            pltpu.VMEM((4, 4, 256, 512), b16),
            pltpu.VMEM((2, 128, 512), b16),
            pltpu.VMEM((2, 128, 512), b16),
            pltpu.VMEM((2, 128, 512), b16),
            pltpu.VMEM((2, 128, 512), b16),
            pltpu.VMEM((4, 256, 128), f32),
            pltpu.VMEM((4, 256, 128), f32),
            pltpu.VMEM((4, 256, 128), f32),
            pltpu.VMEM((2, 256, 128), f32),
            pltpu.VMEM((2, 256, 128), f32),
            pltpu.VMEM((2, 256, 256), f32),
            pltpu.VMEM((512, 4096), b16),
            pltpu.VMEM((512, 4096), b16),
            pltpu.VMEM((32, 4096), b16),
            pltpu.VMEM((4, 4, 32, 1024), b16),
            pltpu.VMEM((4, 4, 32, 1024), b16),
            dma((3,)), dma((3,)), dma((3,)),
            dma((4, 2)), dma((4, 2, 2)), dma((4, 2)), dma((4, 2, 2)),
            dma((4, 4)), dma((4, 4)), dma((4, 4)), dma((4, 4)),
            dma((3,)), dma(()), dma(()),
            dma((4, 4)), dma((4, 4)), dma((4,)), dma((4,)),
        ],
        compiler_params=pltpu.CompilerParams(
            collective_id=0, has_side_effects=True, vmem_limit_bytes=48 * 2**20
        ),
        cost_estimate=pl.CostEstimate(flops=4 * 10**9, bytes_accessed=12 * 2**20, transcendentals=3 * 10**6),
        name="attend",
    )(qn, kn, vn, rows(gn), qb, kb, vb, rows(gb), pn, pb, residual, gain.reshape(1, -1))


def split_up(shard, dim, length):
    dims = shard.shape
    parts = shard.reshape(*dims[:dim], length, dims[dim] // length, *dims[dim + 1 :])
    return jnp.moveaxis(parts, dim, 0)


def sum_at_owner(shard, axis, dim):
    length = lax.axis_size(axis)
    parts = lax.all_to_all(split_up(shard, dim, length), axis, 0, 0, tiled=True)
    return jnp.sum(parts.astype(jnp.float32), axis=0)


def local(
    query_narrow,
    key_narrow,
    value_narrow,
    gates_narrow,
    query_broad,
    key_broad,
    value_broad,
    gates_broad,
    project_narrow,
    project_broad,
    residual,
    norm_gain,
    route_ids,
    route_weight,
    expert_gate,
    expert_up,
    expert_down,
    shared_gate,
    shared_up,
    shared_down,
):
    own_stream, normed = attend(
        query_narrow, key_narrow, value_narrow, gates_narrow,
        query_broad, key_broad, value_broad, gates_broad,
        project_narrow, project_broad, residual, norm_gain,
    )
    shared_hidden = (
        jax.nn.silu(jnp.dot(normed, shared_gate, preferred_element_type=jnp.float32))
        * jnp.dot(normed, shared_up, preferred_element_type=jnp.float32)
    ).astype(jnp.bfloat16)
    sub_rows = route_ids.shape[0]
    own_first = lax.axis_index("tp") * sub_rows
    shared = sum_at_owner(
        jnp.dot(shared_hidden, shared_down, preferred_element_type=jnp.float32).astype(
            jnp.bfloat16
        ),
        "tp",
        0,
    )
    top_count = route_ids.shape[1]
    local_experts = expert_gate.shape[0]
    expert_total = lax.axis_size("sp") * lax.axis_size("tp") * local_experts
    capacity = 2 * sub_rows * top_count // expert_total
    flat_ids = route_ids.reshape(-1)
    one_hot = (flat_ids[:, None] == jnp.arange(expert_total, dtype=jnp.int32)[None, :]).astype(
        jnp.int32
    )
    slot_of = jnp.sum(one_hot * (jnp.cumsum(one_hot, axis=0) - 1), axis=1)
    target = (flat_ids * capacity + slot_of).reshape(sub_rows, top_count)
    slot_total = expert_total * capacity
    matches = target[None, :, :] == jnp.arange(slot_total, dtype=jnp.int32)[:, None, None]
    dispatch = jnp.any(matches, axis=-1).astype(jnp.bfloat16)
    own_normed = lax.dynamic_slice_in_dim(normed, own_first, sub_rows, 0)
    outbound = (
        jnp.dot(dispatch, own_normed, preferred_element_type=jnp.float32)
        .astype(jnp.bfloat16)
        .reshape(expert_total, capacity, -1)
    )
    weight_rounded = route_weight.astype(jnp.bfloat16)
    combiner = jnp.sum(
        jnp.where(matches, weight_rounded[None], jnp.zeros((), jnp.bfloat16)), axis=-1
    ).T
    inbound = lax.all_to_all(outbound, ("sp", "tp"), split_axis=0, concat_axis=0, tiled=True)
    senders = inbound.shape[0] // local_experts
    grouped = inbound.reshape(senders, local_experts, inbound.shape[1], inbound.shape[2])
    gate_out = jnp.einsum(
        "secd,edh->sech", grouped, expert_gate, preferred_element_type=jnp.float32
    )
    up_out = jnp.einsum("secd,edh->sech", grouped, expert_up, preferred_element_type=jnp.float32)
    hidden = (jax.nn.silu(gate_out) * up_out).astype(jnp.bfloat16)
    result = jnp.einsum(
        "sech,ehd->secd", hidden, expert_down, preferred_element_type=jnp.float32
    ).astype(jnp.bfloat16)
    results = result.reshape(inbound.shape)
    returned = lax.all_to_all(results, ("sp", "tp"), split_axis=0, concat_axis=0, tiled=True)
    routed = jnp.dot(combiner, returned.reshape(slot_total, -1), preferred_element_type=jnp.float32)
    return (own_stream + shared + routed).astype(jnp.bfloat16)


def solution(mesh):
    placed = (
        P("sp", "tp"),
        P("sp", "tp"),
        P("sp", "tp"),
        P(None, "tp"),
        P("sp", "tp"),
        P("sp", "tp"),
        P("sp", "tp"),
        P(None, "tp"),
        P("tp", None),
        P("tp", None),
        P("sp", None),
        P(),
        P(("sp", "tp"), None),
        P(("sp", "tp"), None),
        P(("sp", "tp"), None, None),
        P(("sp", "tp"), None, None),
        P(("sp", "tp"), None, None),
        P(None, "tp"),
        P(None, "tp"),
        P("tp", None),
    )
    return jax.shard_map(
        local, mesh=mesh, in_specs=placed, out_specs=P(("sp", "tp"), None), check_vma=False
    )
```

```python
import math

import jax
import jax.numpy as jnp
from jax import lax
from jax.experimental import pallas as pl
from jax.experimental.pallas import tpu as pltpu
from jax.sharding import PartitionSpec as P

norm_epsilon = 1e-06

MESH = pl.DeviceIdType.MESH
LOG2E = math.log2(math.e)


def flash_heads(q_ref, kv, gate_rows, m_ref, l_ref, acc_ref, heads, size, diagonal):
    keys = kv[:, :size]
    values = kv[:, size:]
    rows = q_ref.shape[0] * q_ref.shape[1]
    length = keys.shape[0]
    scale = size ** (-0.5) * LOG2E
    for h in range(heads):
        q = q_ref[:, :, h * size : (h + 1) * size].reshape(rows, size)
        s = lax.dot_general(q, keys, (((1,), (1,)), ((), ())), preferred_element_type=jnp.float32)
        s = s * scale - gate_rows[h : h + 1, :]
        if diagonal:
            at = lax.broadcasted_iota(jnp.int32, (rows, length), 0)
            to = lax.broadcasted_iota(jnp.int32, (rows, length), 1)
            s = jnp.where(to <= at, s, -jnp.inf)
        top = jnp.broadcast_to(jnp.max(s, axis=1, keepdims=True), (rows, 128))
        if not diagonal:
            before = m_ref[h]
            top = jnp.maximum(before, top)
        p = jnp.exp2(s - jnp.concatenate([top] * (length // 128), axis=1))
        total = jnp.broadcast_to(jnp.sum(p, axis=1, keepdims=True), (rows, 128))
        out = jnp.dot(p.astype(jnp.bfloat16), values, preferred_element_type=jnp.float32)
        if not diagonal:
            factor = jnp.exp2(before - top)
            total = total + l_ref[h] * factor
            out = out + acc_ref[h] * jnp.concatenate([factor] * (size // 128), axis=1)
        m_ref[h] = top
        l_ref[h] = total
        acc_ref[h] = out


def layer_kernel(
    qn_in, kn_in, vn_in, gn_in, qb_in, kb_in, vb_in, gb_in, pn_in, pb_in, res_in, gain_in,
    ids_in, rw_in, eg_in, eu_in, ed_in, sg_in, su_in, sd_in,
    out_ref,
    nkv, bkv, qn, qb, attn, held, mn, ln, accn, mb, lb, accb, wn, wb, res, part, got, stream, normed,
    gn, gb, gain, ids, rw, wgu, wd, sgu, sd, codes, dmat, cmat, outb, inb, back, ret, gu, mine,
    theirs, from_pair, part2, got2,
    own_sem, load_sem, own_send, n1_send, n1_recv, b1_send, b1_recv, n2_send, n2_recv, b2_send,
    b2_recv, q_recv, swap_send, swap_recv, r_send, r_recv, a_send, a_recv,
    c_send, c_recv, p_send, p_recv, d_send, d_recv, e_send, e_recv, t_send, t_recv, s_send, s_recv,
):
    sp = lax.axis_index("sp")
    tp = lax.axis_index("tp")
    z = sp // 8
    y = (sp // 2) % 4
    c = sp % 2
    half = pl.ds(pl.multiple_of(c * 128, 128), 128)

    def at(zz, yy, cc):
        return (zz * 8 + yy * 2 + cc, tp)

    barrier = pltpu.get_barrier_semaphore()

    def greet(to):
        pl.semaphore_signal(barrier, inc=1, device_id=to, device_id_type=MESH)

    def greet_chip(t, carry):
        greet(at(lax.rem(z + t // 4, 4), lax.rem(y + t % 4, 4), c))
        return carry

    lax.fori_loop(1, 16, greet_chip, 0)
    for step in range(1, 4):
        greet(at(lax.rem(z + step, 4), y, 1 - c))
        greet(at(z, lax.rem(y + step, 4), 1 - c))
        for cc in range(2):
            greet((z * 8 + y * 2 + cc, lax.rem(tp + step, 4)))
    greet(at(z, y, 1 - c))

    loads = [
        (gn_in, gn), (gb_in, gb), (ids_in, ids), (rw_in, rw), (gain_in, gain),
        (res_in.at[pl.ds(pl.multiple_of(tp * 32, 32), 32)], res),
        (pn_in, wn), (pb_in, wb),
        (sg_in, sgu.at[:, pl.ds(0, 256)]), (su_in, sgu.at[:, pl.ds(256, 256)]), (sd_in, sd),
        (eg_in.at[0], wgu.at[:, pl.ds(0, 256)]), (eu_in.at[0], wgu.at[:, pl.ds(256, 256)]),
        (ed_in.at[0], wd),
    ]

    def load(i):
        return pltpu.make_async_copy(loads[i][0], loads[i][1], load_sem.at[i])

    for i in range(len(loads)):
        load(i).start()
    pl.semaphore_wait(barrier, 28)

    def remote(src, dst, send, recv, to):
        return pltpu.make_async_remote_copy(
            src_ref=src, dst_ref=dst, send_sem=send, recv_sem=recv, device_id=to, device_id_type=MESH
        )

    nslot = ((kn_in, pl.ds(0, 128)), (vn_in, pl.ds(128, 128)))
    bslot = ((kb_in, pl.ds(0, 256)), (vb_in, pl.ds(256, 256)))

    def n_own(i):
        return nslot[i][0], nkv.at[z, y, half, nslot[i][1]]

    def b_own(i):
        return bslot[i][0], bkv.at[z, y, half, bslot[i][1]]

    n_pairs = [(lambda i=i: n_own(i)) for i in range(2)] + [lambda: (qn_in, qn.at[c])]
    b_pairs = [(lambda i=i: b_own(i)) for i in range(2)] + [lambda: (qb_in, qb.at[c])]

    for role, own, other in ((0, n_pairs, b_pairs), (1, b_pairs, n_pairs)):

        @pl.when(c == role)
        def _(own=own, other=other, role=role):
            for i in range(3):
                src, dst = other[i]()
                remote(src, dst, own_send.at[i], q_recv.at[i], at(z, y, 1 - role)).start()
            for i in range(3):
                src, dst = own[i]()
                pltpu.make_async_copy(src, dst, own_sem.at[i]).start()

    for step in range(1, 4):

        @pl.when(z + step < 4)
        def _(step=step):
            for i in range(2):
                src, dst = n_own(i)
                remote(src, dst, n1_send.at[step, i], n1_recv.at[z, c, i], at(z + step, y, 0)).start()

        for i in range(2):
            src, dst = b_own(i)
            remote(
                src, dst, b1_send.at[step, i], b1_recv.at[y, c, i], at(z, lax.rem(y + step, 4), 1)
            ).start()

    me = c * 4 + tp
    for i in range(4):
        load(i).wait()
    lane = lax.broadcasted_iota(jnp.int32, (8, 128), 1)
    row = lax.broadcasted_iota(jnp.int32, (32, 128), 0)
    spot = (lax.broadcasted_iota(jnp.int32, (32, 128), 1) == row + tp * 32).astype(jnp.bfloat16)
    put = lambda a: jnp.dot(a.astype(jnp.bfloat16), spot, preferred_element_type=jnp.float32)
    placed_ids = put(ids[...].astype(jnp.float32))
    placed_rw = put(rw[...])
    inside = (lane[:4] // 32) == tp
    key_ids = jnp.where(inside, placed_ids, -1.0)
    names = lax.broadcasted_iota(jnp.int32, (128, 128), 0).astype(jnp.float32)
    later = (
        lax.broadcasted_iota(jnp.int32, (128, 128), 0) < lax.broadcasted_iota(jnp.int32, (128, 128), 1)
    ).astype(jnp.bfloat16)
    hits = [jnp.where(key_ids[k : k + 1] == names, 1.0, 0.0) for k in range(4)]
    before = jnp.dot(
        (hits[0] + hits[1] + hits[2] + hits[3]).astype(jnp.bfloat16), later,
        preferred_element_type=jnp.float32,
    )
    for k in range(4):
        rank = jnp.sum(hits[k] * before, axis=0, keepdims=True)
        codes[me, k : k + 1] = placed_ids[k : k + 1] * 2.0 + rank
        codes[me, 4 + k : 5 + k] = placed_rw[k : k + 1]

    def code(t):
        to = lax.rem(me + t, 8)
        return remote(
            codes.at[me], codes.at[me], c_send.at[t], c_recv.at[t], (z * 8 + y * 2 + to // 4, to % 4)
        )

    for t in range(1, 8):
        code(t).start()

    def gate_rows(ref, zz, yy):
        return ref[:, pl.ds(pl.multiple_of((zz * 4 + yy) * 256, 256), 256)] * LOG2E

    def own_wait(role, own, other):
        for i in range(3):
            src, dst = own[i]()
            pltpu.make_async_copy(src, dst, own_sem.at[i]).wait()
        oc = 1 - role
        ohalf = pl.ds(oc * 128, 128)
        if role == 0:
            dsts = [nkv.at[z, y, ohalf, nslot[i][1]] for i in range(2)] + [qn.at[oc]]
            srcs = [kn_in, vn_in, qn_in]
        else:
            dsts = [bkv.at[z, y, ohalf, bslot[i][1]] for i in range(2)] + [qb.at[oc]]
            srcs = [kb_in, vb_in, qb_in]
        for i in range(3):
            remote(srcs[i], dsts[i], own_send.at[i], q_recv.at[i], at(z, y, oc)).wait_recv()

    @pl.when(c == 0)
    def _():
        own_wait(0, n_pairs, b_pairs)

        def n2(zz, step, yy=None):
            to = y + step if yy is None else yy
            return remote(
                nkv.at[zz, y], nkv.at[zz, y], n2_send.at[zz, step], n2_recv.at[zz, y],
                at(z, lax.rem(y + step, 4), 0),
            )

        def send_on(zz):
            for step in range(1, 4):
                @pl.when((zz < z) | (y + step < 4))
                def _(step=step):
                    n2(zz, step).start()

        def block(zz, yy, diagonal):
            flash_heads(
                qn, nkv[zz, yy], gate_rows(gn, zz, yy), mn, ln, accn, 4, 128, diagonal
            )

        send_on(z)
        block(z, y, True)

        def column(t, carry):
            zz = z - t
            for cc in range(2):
                for i in range(2):
                    remote(
                        nslot[i][0], nkv.at[zz, y, pl.ds(cc * 128, 128), nslot[i][1]],
                        n1_send.at[1, i], n1_recv.at[zz, cc, i], at(zz, y, 0),
                    ).wait_recv()
            send_on(zz)
            block(zz, y, False)
            return carry

        lax.fori_loop(1, z + 1, column, 0)

        def rest(t, carry):
            zz = z - t // 3
            yy = lax.rem(y + t % 3 + 1, 4)

            @pl.when((zz < z) | (yy < y))
            def _():
                remote(
                    nkv.at[zz, yy], nkv.at[zz, yy], n2_send.at[zz, 1], n2_recv.at[zz, yy],
                    at(z, yy, 0),
                ).wait_recv()
                block(zz, yy, False)

            return carry

        lax.fori_loop(0, 3 * (z + 1), rest, 0)
        for h in range(4):
            out = (accn[h] / ln[h]).astype(jnp.bfloat16)
            held[:, :, h * 128 : (h + 1) * 128] = out.reshape(2, 128, 128)
        remote(
            held.at[1], attn.at[0], swap_send, swap_recv, at(z, y, 1)
        ).start()
        attn[0] = held[0]

        def drain(t, carry):
            for step in range(1, 4):
                @pl.when((t < z) | (y + step < 4))
                def _(step=step):
                    n2(t, step).wait_send()
            return carry

        lax.fori_loop(0, z + 1, drain, 0)

    @pl.when(c == 1)
    def _():
        own_wait(1, b_pairs, n_pairs)

        def b2(yy, step):
            return remote(
                bkv.at[z, yy], bkv.at[z, yy], b2_send.at[yy, step], b2_recv.at[z, yy],
                at(z + step, y, 1),
            )

        def send_on(yy):
            for step in range(1, 4):
                @pl.when(z + step < 4)
                def _(step=step):
                    b2(yy, step).start()

        def block(zz, yy, diagonal):
            flash_heads(qb, bkv[zz, yy], gate_rows(gb, zz, yy), mb, lb, accb, 2, 256, diagonal)

        send_on(y)
        block(z, y, True)

        def row(t, carry):
            yy = lax.rem(y + t, 4)
            for cc in range(2):
                for i in range(2):
                    remote(
                        bslot[i][0], bkv.at[z, yy, pl.ds(cc * 128, 128), bslot[i][1]],
                        b1_send.at[1, i], b1_recv.at[yy, cc, i], at(z, yy, 1),
                    ).wait_recv()
            send_on(yy)

            @pl.when(yy < y)
            def _():
                block(z, yy, False)

            return carry

        lax.fori_loop(1, 4, row, 0)

        def rest(t, carry):
            zz = z - 1 - t // 4
            yy = lax.rem(y + t, 4)
            remote(
                bkv.at[zz, yy], bkv.at[zz, yy], b2_send.at[yy, 1], b2_recv.at[zz, yy], at(zz, y, 1)
            ).wait_recv()
            block(zz, yy, False)
            return carry

        lax.fori_loop(0, 4 * z, rest, 0)
        for h in range(2):
            out = (accb[h] / jnp.concatenate([lb[h]] * 2, axis=1)).astype(jnp.bfloat16)
            held[:, :, h * 256 : (h + 1) * 256] = out.reshape(2, 128, 256)
        remote(
            held.at[0], attn.at[1], swap_send, swap_recv, at(z, y, 0)
        ).start()
        attn[1] = held[1]

        def drain(t, carry):
            for step in range(1, 4):
                @pl.when(z + step < 4)
                def _(step=step):
                    b2(t, step).wait_send()
            return carry

        lax.fori_loop(0, 4, drain, 0)

    for i in range(3):
        src, dst = n_pairs[i]() if i < 2 else n_pairs[2]()

        @pl.when(c == 1)
        def _(i=i):
            src, dst = n_pairs[i]()
            remote(src, dst, own_send.at[i], q_recv.at[i], at(z, y, 0)).wait_send()

        @pl.when(c == 0)
        def _(i=i):
            src, dst = b_pairs[i]()
            remote(src, dst, own_send.at[i], q_recv.at[i], at(z, y, 1)).wait_send()

    for step in range(1, 4):

        @pl.when(z + step < 4)
        def _(step=step):
            for i in range(2):
                src, dst = n_own(i)
                remote(src, dst, n1_send.at[step, i], n1_recv.at[z, c, i], at(z + step, y, 0)).wait_send()

        for i in range(2):
            src, dst = b_own(i)
            remote(
                src, dst, b1_send.at[step, i], b1_recv.at[y, c, i], at(z, lax.rem(y + step, 4), 1)
            ).wait_send()

    remote(held.at[1 - c], attn.at[1 - c], swap_send, swap_recv, at(z, y, 1 - c)).wait()
    for i in range(4, 8):
        load(i).wait()

    CH = 1024
    NC = 4096 // CH

    def sent(n, step):
        to = lax.rem(tp + step, 4)
        return remote(
            part.at[n, to], got.at[n, tp], r_send.at[n, step], r_recv.at[n, tp], (sp, to)
        )

    for n in range(NC):
        cols = pl.ds(n * CH, CH)
        p = jnp.dot(attn[0], wn[:, cols], preferred_element_type=jnp.float32)
        p = p + jnp.dot(attn[1], wb[:, cols], preferred_element_type=jnp.float32)
        part[n] = p.astype(jnp.bfloat16).reshape(4, 32, CH)
        for step in range(1, 4):
            sent(n, step).start()

    squares = jnp.zeros((32, 128), jnp.float32)
    for n in range(NC):
        for step in range(1, 4):
            frm = lax.rem(tp + step, 4)
            remote(
                part.at[n, frm], got.at[n, frm], r_send.at[n, step], r_recv.at[n, frm], (sp, frm)
            ).wait_recv()
        cols = pl.ds(n * CH, CH)
        total = res[:, cols].astype(jnp.float32) + part[n, tp].astype(jnp.float32)
        for step in range(1, 4):
            total = total + got[n, lax.rem(tp + step, 4)].astype(jnp.float32)
        stream[:, cols] = total
        sq = total * total
        for k in range(CH // 128):
            squares = squares + sq[:, k * 128 : (k + 1) * 128]
    mean = jnp.sum(squares, axis=1, keepdims=True) * (1.0 / 4096)
    rate = lax.rsqrt(mean + norm_epsilon)
    rows_of = lambda who: pl.ds(pl.multiple_of(who * 32, 32), 32)
    for n in range(NC):
        cols = pl.ds(n * CH, CH)
        normed[c, rows_of(tp), cols] = (stream[:, cols] * rate * gain[:, cols]).astype(jnp.bfloat16)

    def gather(step):
        to = lax.rem(tp + step, 4)
        block = normed.at[c, rows_of(tp)]
        return remote(block, block, a_send.at[step], a_recv.at[step], (sp, to))

    def pair(who):
        block = normed.at[c, rows_of(who)]
        return remote(block, block, p_send.at[who], p_recv.at[who], at(z, y, 1 - c))

    for step in range(1, 4):
        gather(step).start()
    pair(tp).start()

    for t in range(1, 8):
        code(t).wait_recv()
    halves = [codes[h * 4] + codes[h * 4 + 1] + codes[h * 4 + 2] + codes[h * 4 + 3] for h in range(2)]
    table = jnp.concatenate(halves, axis=1)
    slot = lax.broadcasted_iota(jnp.int32, (256, 256), 0)
    token = lax.broadcasted_iota(jnp.int32, (256, 256), 1)
    wanted = (((slot // 16) * 2 + c) * 4 + tp) * 2 + slot % 2
    wanted = jnp.where((slot // 2) % 8 == token // 32, wanted, -1).astype(jnp.float32)
    picks = jnp.zeros((256, 256), jnp.float32)
    pays = jnp.zeros((256, 256), jnp.float32)
    for k in range(4):
        same = table[k : k + 1] == wanted
        picks = picks + jnp.where(same, 1.0, 0.0)
        pays = pays + jnp.where(same, table[4 + k : 5 + k], 0.0)
    dmat[...] = picks.astype(jnp.bfloat16)
    cmat[...] = pays.T.reshape(2, 128, 256).astype(jnp.bfloat16)

    for step in range(1, 4):
        gather(step).wait_recv()
    for step in range(1, 4):
        pair(lax.rem(tp + step, 4)).start()
    for who in range(4):
        block = normed.at[1 - c, pl.ds(who * 32, 32)]
        remote(block, block, p_send.at[who], p_recv.at[who], at(z, y, 1 - c)).wait_recv()

    chip = z * 4 + y

    def slots(src, dst, send, recv, n):
        def one(t, carry):
            zz, yy = lax.rem(z + t // 4, 4), lax.rem(y + t % 4, 4)
            remote(
                src.at[n, zz * 4 + yy], dst.at[n, chip], send.at[n], recv.at[n], at(zz, yy, c)
            ).start()
            return carry

        lax.fori_loop(1, 16, one, 0)

    def all_of(ref, sem, n):
        block = ref.at[n, pl.ds(0, 15)]
        return pltpu.make_async_copy(block, block, sem.at[n])

    for n in range(NC):
        cols = pl.ds(n * CH, CH)
        rows = normed[:, :, cols].reshape(256, CH)
        picked = jnp.dot(dmat[...], rows, preferred_element_type=jnp.float32).astype(jnp.bfloat16)
        outb[n] = picked.reshape(16, 16, CH)
        slots(outb, inb, d_send, d_recv, n)
        inb[n, chip] = outb[n, chip]

    for i in range(8, 14):
        load(i).wait()
    both = jnp.dot(normed[c], sgu[...], preferred_element_type=jnp.float32)
    gate, up = both[:, :256], both[:, 256:]
    hidden = (gate / (1.0 + jnp.exp(-gate)) * up).astype(jnp.bfloat16)
    for n in range(NC):
        mine[n] = jnp.dot(hidden, sd[:, n * CH : (n + 1) * CH], preferred_element_type=jnp.float32)

    for n in range(NC):
        all_of(inb, d_recv, n).wait()
        more = jnp.dot(
            inb[n].reshape(256, CH), wgu[n * CH : (n + 1) * CH, :], preferred_element_type=jnp.float32
        )
        gu[...] = more if n == 0 else gu[...] + more
    gate, up = gu[:, :256], gu[:, 256:]
    hidden = (gate / (1.0 + jnp.exp(-gate)) * up).astype(jnp.bfloat16)
    for n in range(NC):
        made = jnp.dot(hidden, wd[:, n * CH : (n + 1) * CH], preferred_element_type=jnp.float32)
        back[n] = made.astype(jnp.bfloat16).reshape(16, 16, CH)
        slots(back, ret, e_send, e_recv, n)
        ret[n, chip] = back[n, chip]

    def to_pair(n):
        return remote(theirs.at[n], from_pair.at[n], t_send.at[n], t_recv.at[n], at(z, y, 1 - c))

    def to_owner(n, step):
        to = lax.rem(tp + step, 4)
        return remote(
            part2.at[n, to], got2.at[n, step], s_send.at[n, step], s_recv.at[n, step], (sp, to)
        )

    for i in range(NC + 2):
        if i < NC:
            all_of(ret, e_recv, i).wait()
            rows = ret[i].reshape(256, CH)
            theirs[i] = jnp.dot(cmat[1 - c], rows, preferred_element_type=jnp.float32).astype(
                jnp.bfloat16
            )
            to_pair(i).start()
            mine[i] = mine[i] + jnp.dot(cmat[c], rows, preferred_element_type=jnp.float32)
        if 0 <= i - 1 < NC:
            n = i - 1
            to_pair(n).wait_recv()
            both = mine[n] + from_pair[n].astype(jnp.float32)
            part2[n] = both.astype(jnp.bfloat16).reshape(4, 32, CH)
            for step in range(1, 4):
                to_owner(n, step).start()
        if 0 <= i - 2:
            n = i - 2
            for step in range(1, 4):
                to_owner(n, step).wait_recv()
            total = stream[:, n * CH : (n + 1) * CH] + part2[n, tp].astype(jnp.float32)
            for step in range(1, 4):
                total = total + got2[n, step].astype(jnp.float32)
            out_ref[:, n * CH : (n + 1) * CH] = total.astype(jnp.bfloat16)

    for t in range(1, 8):
        code(t).wait_send()
    for step in range(1, 4):
        gather(step).wait_send()
    for who in range(4):
        pair(who).wait_send()
    for n in range(NC):
        for step in range(1, 4):
            sent(n, step).wait_send()
            to_owner(n, step).wait_send()
        all_of(outb, d_send, n).wait()
        all_of(back, e_send, n).wait()
        to_pair(n).wait_send()


def layer(*args):
    any_ = pl.BlockSpec(memory_space=pl.ANY)
    dma = pltpu.SemaphoreType.DMA
    f32, b16 = jnp.float32, jnp.bfloat16
    vm = pltpu.VMEM
    return pl.pallas_call(
        layer_kernel,
        out_shape=jax.ShapeDtypeStruct((32, 4096), b16),
        in_specs=[any_] * len(args),
        out_specs=pl.BlockSpec(memory_space=pltpu.VMEM),
        scratch_shapes=[
            vm((4, 4, 256, 256), b16), vm((4, 4, 256, 512), b16),
            vm((2, 128, 512), b16), vm((2, 128, 512), b16), vm((2, 128, 512), b16), vm((2, 128, 512), b16),
            vm((4, 256, 128), f32), vm((4, 256, 128), f32), vm((4, 256, 128), f32),
            vm((2, 256, 128), f32), vm((2, 256, 128), f32), vm((2, 256, 256), f32),
            vm((512, 4096), b16), vm((512, 4096), b16), vm((32, 4096), b16),
            vm((4, 4, 32, 1024), b16), vm((4, 4, 32, 1024), b16), vm((32, 4096), f32), vm((2, 128, 4096), b16),
            vm((4, 4096), f32), vm((2, 4096), f32), vm((1, 4096), f32), vm((4, 32), jnp.int32), vm((4, 32), f32),
            vm((4096, 512), b16), vm((256, 4096), b16), vm((4096, 512), b16), vm((256, 4096), b16),
            vm((8, 8, 128), f32), vm((256, 256), b16), vm((2, 128, 256), b16),
            vm((4, 16, 16, 1024), b16), vm((4, 16, 16, 1024), b16), vm((4, 16, 16, 1024), b16), vm((4, 16, 16, 1024), b16),
            vm((256, 512), f32), vm((4, 128, 1024), f32),
            vm((4, 128, 1024), b16), vm((4, 128, 1024), b16), vm((4, 4, 32, 1024), b16), vm((4, 4, 32, 1024), b16),
            dma((3,)), dma((14,)), dma((3,)),
            dma((4, 2)), dma((4, 2, 2)), dma((4, 2)), dma((4, 2, 2)),
            dma((4, 4)), dma((4, 4)), dma((4, 4)), dma((4, 4)),
            dma((3,)), dma(()), dma(()),
            dma((4, 4)), dma((4, 4)), dma((4,)), dma((4,)),
            dma((8,)), dma((8,)), dma((4,)), dma((4,)),
            dma((4,)), dma((4,)), dma((4,)), dma((4,)), dma((4,)), dma((4,)), dma((4, 4)), dma((4, 4)),
        ],
        compiler_params=pltpu.CompilerParams(
            collective_id=0, has_side_effects=True, vmem_limit_bytes=67043328
        ),
        name="layer",
    )(*args)


def local(
    query_narrow, key_narrow, value_narrow, gates_narrow, query_broad, key_broad, value_broad,
    gates_broad, project_narrow, project_broad, residual, norm_gain, route_ids, route_weight,
    expert_gate, expert_up, expert_down, shared_gate, shared_up, shared_down,
):
    return layer(
        query_narrow, key_narrow, value_narrow, gates_narrow.T, query_broad, key_broad, value_broad,
        gates_broad.T, project_narrow, project_broad, residual, norm_gain.reshape(1, -1), route_ids.T,
        route_weight.T, expert_gate, expert_up, expert_down, shared_gate, shared_up, shared_down,
    )


def solution(mesh):
    placed = (
        P("sp", "tp"),
        P("sp", "tp"),
        P("sp", "tp"),
        P(None, "tp"),
        P("sp", "tp"),
        P("sp", "tp"),
        P("sp", "tp"),
        P(None, "tp"),
        P("tp", None),
        P("tp", None),
        P("sp", None),
        P(),
        P(("sp", "tp"), None),
        P(("sp", "tp"), None),
        P(("sp", "tp"), None, None),
        P(("sp", "tp"), None, None),
        P(("sp", "tp"), None, None),
        P(None, "tp"),
        P(None, "tp"),
        P("tp", None),
    )
    return jax.shard_map(
        local, mesh=mesh, in_specs=placed, out_specs=P(("sp", "tp"), None), check_vma=False
    )
```

```python
import math

import jax
import jax.numpy as jnp
from jax import lax
from jax.experimental import pallas as pl
from jax.experimental.pallas import tpu as pltpu
from jax.sharding import PartitionSpec as P

norm_epsilon = 1e-06
COLUMNS = 512
BLOCKS = 4096 // COLUMNS
BEHIND = 4
FAR_FIRST = (
    (2, 2), (2, 3), (3, 2), (2, 1), (1, 2), (2, 0), (0, 2), (3, 1), (1, 3), (3, 3), (1, 1), (3, 0), (0, 3),
    (1, 0), (0, 1),
)

MESH = pl.DeviceIdType.MESH
LOG2E = math.log2(math.e)


def flash_heads(q_ref, kv, gate_rows, m_ref, l_ref, acc_ref, heads, size, diagonal):
    keys = kv[:, :size]
    values = kv[:, size:]
    rows = q_ref.shape[0] * q_ref.shape[1]
    length = keys.shape[0]
    scale = size ** (-0.5) * LOG2E
    for h in range(heads):
        q = q_ref[:, :, h * size : (h + 1) * size].reshape(rows, size)
        s = lax.dot_general(q, keys, (((1,), (1,)), ((), ())), preferred_element_type=jnp.float32)
        s = s * scale - gate_rows[h : h + 1, :]
        if diagonal:
            at = lax.broadcasted_iota(jnp.int32, (rows, length), 0)
            to = lax.broadcasted_iota(jnp.int32, (rows, length), 1)
            s = jnp.where(to <= at, s, -jnp.inf)
        top = jnp.broadcast_to(jnp.max(s, axis=1, keepdims=True), (rows, 128))
        if not diagonal:
            before = m_ref[h]
            top = jnp.maximum(before, top)
        p = jnp.exp2(s - jnp.concatenate([top] * (length // 128), axis=1))
        total = jnp.broadcast_to(jnp.sum(p, axis=1, keepdims=True), (rows, 128))
        out = jnp.dot(p.astype(jnp.bfloat16), values, preferred_element_type=jnp.float32)
        if not diagonal:
            factor = jnp.exp2(before - top)
            total = total + l_ref[h] * factor
            out = out + acc_ref[h] * jnp.concatenate([factor] * (size // 128), axis=1)
        m_ref[h] = top
        l_ref[h] = total
        acc_ref[h] = out


def layer_kernel(
    qn_in, kn_in, vn_in, gn_in, qb_in, kb_in, vb_in, gb_in, pn_in, pb_in, res_in, gain_in,
    ids_in, rw_in, eg_in, eu_in, ed_in, sg_in, su_in, sd_in,
    out_ref,
    nkv, bkv, qn, qb, attn, held, mn, ln, accn, mb, lb, accb, wn, wb, res, part, got, stream, normed,
    gn, gb, gain, ids, rw, wgu, wd, sgu, sd, codes, scales, rout, rin, dmat, cmat, outb, inb, back, ret, gu, mine,
    theirs, from_pair, part2, got2, part3, got3,
    own_sem, load_sem, own_send, n1_send, n1_recv, b1_send, b1_recv, n2_send, n2_recv, b2_send,
    b2_recv, q_recv, swap_send, swap_recv, r_send, r_recv, a_send, a_recv,
    c_send, c_recv, p_send, p_recv, d_send, d_recv, e_send, e_recv, t_send, t_recv, s_send, s_recv,
    g_send, g_recv, h_send, h_recv, t3_send, t3_recv,
):
    sp = lax.axis_index("sp")
    tp = lax.axis_index("tp")
    z = sp // 8
    y = (sp // 2) % 4
    c = sp % 2
    half = pl.ds(pl.multiple_of(c * 128, 128), 128)

    def at(zz, yy, cc):
        return (zz * 8 + yy * 2 + cc, tp)

    barrier = pltpu.get_barrier_semaphore()

    def greet(to):
        pl.semaphore_signal(barrier, inc=1, device_id=to, device_id_type=MESH)

    def greet_chip(t, carry):
        greet(at(lax.rem(z + t // 4, 4), lax.rem(y + t % 4, 4), c))
        return carry

    lax.fori_loop(1, 16, greet_chip, 0)
    for step in range(1, 4):
        greet(at(lax.rem(z + step, 4), y, 1 - c))
        greet(at(z, lax.rem(y + step, 4), 1 - c))
        for cc in range(2):
            greet((z * 8 + y * 2 + cc, lax.rem(tp + step, 4)))
    greet(at(z, y, 1 - c))

    loads = [
        (gn_in, gn), (gb_in, gb), (ids_in, ids), (rw_in, rw), (gain_in, gain),
        (res_in.at[pl.ds(pl.multiple_of(tp * 32, 32), 32)], res),
        (pn_in, wn), (pb_in, wb),
        (sg_in, sgu.at[:, pl.ds(0, 256)]), (su_in, sgu.at[:, pl.ds(256, 256)]), (sd_in, sd),
        (eg_in.at[0], wgu.at[:, pl.ds(0, 256)]), (eu_in.at[0], wgu.at[:, pl.ds(256, 256)]),
        (ed_in.at[0], wd),
    ]

    def load(i):
        return pltpu.make_async_copy(loads[i][0], loads[i][1], load_sem.at[i])

    for i in range(6):
        load(i).start()
    pl.semaphore_wait(barrier, 28)

    def remote(src, dst, send, recv, to):
        return pltpu.make_async_remote_copy(
            src_ref=src, dst_ref=dst, send_sem=send, recv_sem=recv, device_id=to, device_id_type=MESH
        )

    own_n = nkv.at[z, y, half]
    own_b = bkv.at[z, y, half]
    owns = (
        (kn_in, nkv.at[z, y, half, pl.ds(0, 128)]), (vn_in, nkv.at[z, y, half, pl.ds(128, 128)]),
        (kb_in, bkv.at[z, y, half, pl.ds(0, 256)]), (vb_in, bkv.at[z, y, half, pl.ds(256, 256)]),
    )

    def own(i):
        return pltpu.make_async_copy(owns[i][0], owns[i][1], own_sem.at[i])

    q_sides = ((qn_in, qn), (qb_in, qb))

    def q_own(role):
        return pltpu.make_async_copy(q_sides[role][0], q_sides[role][1].at[c], own_sem.at[4])

    def q_over(role):
        return remote(
            q_sides[role][0], q_sides[role][1].at[c], own_send.at[0], q_recv.at[0], at(z, y, role)
        )

    def kv_over(role):
        block = (own_n, own_b)[role]
        return remote(block, block, own_send.at[1], q_recv.at[1], at(z, y, role))

    def n1(step):
        return remote(own_n, own_n, n1_send.at[step], n1_recv.at[z, c], at(z + step, y, 0))

    def b1(step):
        return remote(
            own_b, own_b, b1_send.at[step], b1_recv.at[y, c], at(z, lax.rem(y + step, 4), 1)
        )

    for i in range(4):
        own(i).start()
    for role in range(2):

        @pl.when(c == role)
        def _(role=role):
            q_own(role).start()
            q_over(1 - role).start()

    for i in range(4):
        own(i).wait()
    for step in (1, 3, 2):
        b1(step).start()

        @pl.when(z + step < 4)
        def _(step=step):
            n1(step).start()

    for role in range(2):

        @pl.when(c == role)
        def _(role=role):
            kv_over(1 - role).start()

    me = c * 4 + tp
    for i in range(4):
        load(i).wait()
    lane = lax.broadcasted_iota(jnp.int32, (8, 128), 1)
    row = lax.broadcasted_iota(jnp.int32, (32, 128), 0)
    place = lax.broadcasted_iota(jnp.int32, (32, 128), 1) == row + tp * 32
    spot = place.astype(jnp.bfloat16)
    put = lambda a: jnp.dot(a.astype(jnp.bfloat16), spot, preferred_element_type=jnp.float32)
    placed_ids = put(ids[...].astype(jnp.float32))
    placed_rw = put(rw[...])
    inside = (lane[:4] // 32) == tp
    key_ids = jnp.where(inside, placed_ids, -1.0)
    names = lax.broadcasted_iota(jnp.int32, (128, 128), 0).astype(jnp.float32)
    later = (
        lax.broadcasted_iota(jnp.int32, (128, 128), 0) < lax.broadcasted_iota(jnp.int32, (128, 128), 1)
    ).astype(jnp.bfloat16)
    hits = [jnp.where(key_ids[k : k + 1] == names, 1.0, 0.0) for k in range(4)]
    before = jnp.dot(
        (hits[0] + hits[1] + hits[2] + hits[3]).astype(jnp.bfloat16), later,
        preferred_element_type=jnp.float32,
    )
    for k in range(4):
        rank = jnp.sum(hits[k] * before, axis=0, keepdims=True)
        codes[me, k : k + 1] = placed_ids[k : k + 1] * 2.0 + rank
        codes[me, 4 + k : 5 + k] = placed_rw[k : k + 1]

    def code(t):
        to = lax.rem(me + t, 8)
        return remote(
            codes.at[me], codes.at[me], c_send.at[t], c_recv.at[t], (z * 8 + y * 2 + to // 4, to % 4)
        )

    for t in range(1, 8):
        code(t).start()

    def gate_rows(ref, zz, yy):
        return ref[:, pl.ds(pl.multiple_of((zz * 4 + yy) * 256, 256), 256)] * LOG2E

    def own_wait(role):
        block = (nkv, bkv)[role].at[z, y, pl.ds((1 - role) * 128, 128)]
        remote(block, block, own_send.at[1], q_recv.at[1], at(z, y, 1 - role)).wait_recv()

    def q_wait(role):
        q_own(role).wait()
        there = q_sides[role][1].at[1 - c]
        remote(there, there, own_send.at[0], q_recv.at[0], at(z, y, 1 - role)).wait_recv()

    def n2(zz, step):
        return remote(
            nkv.at[zz, y], nkv.at[zz, y], n2_send.at[zz, step], n2_recv.at[zz, y],
            at(z, lax.rem(y + step, 4), 0),
        )

    def b2(yy, step):
        return remote(
            bkv.at[z, yy], bkv.at[z, yy], b2_send.at[yy, step], b2_recv.at[z, yy],
            at(z + step, y, 1),
        )

    @pl.when(c == 0)
    def _():
        own_wait(0)
        q_wait(0)

        def send_on(zz):
            for step in range(1, 4):
                @pl.when((zz < z) | (y + step < 4))
                def _(step=step):
                    n2(zz, step).start()

        def block(zz, yy, diagonal):
            flash_heads(
                qn, nkv[zz, yy], gate_rows(gn, zz, yy), mn, ln, accn, 4, 128, diagonal
            )

        block(z, y, True)
        for step in range(1, 4):
            b1(step).wait_send()
        send_on(z)

        def column(t, carry):
            zz = z - t
            for cc in range(2):
                there = nkv.at[zz, y, pl.ds(cc * 128, 128)]
                remote(there, there, n1_send.at[1], n1_recv.at[zz, cc], at(zz, y, 0)).wait_recv()
            send_on(zz)
            return carry

        lax.fori_loop(1, z + 1, column, 0)
        for i in range(6, 14):
            load(i).start()

        def column_block(t, carry):
            block(z - t, y, False)
            return carry

        lax.fori_loop(1, z + 1, column_block, 0)

        def rest(t, carry):
            zz = z - t // 3
            yy = lax.rem(y + t % 3 + 1, 4)

            @pl.when((zz < z) | (yy < y))
            def _():
                remote(
                    nkv.at[zz, yy], nkv.at[zz, yy], n2_send.at[zz, 1], n2_recv.at[zz, yy],
                    at(z, yy, 0),
                ).wait_recv()
                block(zz, yy, False)

            return carry

        lax.fori_loop(0, 3 * (z + 1), rest, 0)
        for h in range(4):
            out = (accn[h] / ln[h]).astype(jnp.bfloat16)
            held[:, :, h * 128 : (h + 1) * 128] = out.reshape(2, 128, 128)
        remote(
            held.at[1], attn.at[0], swap_send, swap_recv, at(z, y, 1)
        ).start()
        attn[0] = held[0]

    @pl.when(c == 1)
    def _():
        own_wait(1)

        def send_on(yy):
            for step in range(1, 4):
                @pl.when(z + step < 4)
                def _(step=step):
                    b2(yy, step).start()

        def block(zz, yy, diagonal):
            flash_heads(qb, bkv[zz, yy], gate_rows(gb, zz, yy), mb, lb, accb, 2, 256, diagonal)

        send_on(y)
        q_wait(1)
        block(z, y, True)

        def turn(t):
            return lax.rem(y + jnp.where(t == 2, 3, jnp.where(t == 3, 2, t)), 4)

        def row(t, carry):
            yy = turn(t)
            for cc in range(2):
                there = bkv.at[z, yy, pl.ds(cc * 128, 128)]
                remote(there, there, b1_send.at[1], b1_recv.at[yy, cc], at(z, yy, 1)).wait_recv()
            send_on(yy)
            return carry

        lax.fori_loop(1, 4, row, 0)
        for i in range(6, 14):
            load(i).start()

        def row_block(t, carry):
            block(z, t, False)
            return carry

        lax.fori_loop(0, y, row_block, 0)

        def rest(t, carry):
            yy = turn(t)

            def one(k, inner):
                zz = z - k
                remote(
                    bkv.at[zz, yy], bkv.at[zz, yy], b2_send.at[yy, 1], b2_recv.at[zz, yy],
                    at(zz, y, 1),
                ).wait_recv()
                block(zz, yy, False)
                return inner

            return lax.fori_loop(1, z + 1, one, carry)

        lax.fori_loop(0, 4, rest, 0)
        for h in range(2):
            out = (accb[h] / jnp.concatenate([lb[h]] * 2, axis=1)).astype(jnp.bfloat16)
            held[:, :, h * 256 : (h + 1) * 256] = out.reshape(2, 128, 256)
        remote(
            held.at[0], attn.at[1], swap_send, swap_recv, at(z, y, 0)
        ).start()
        attn[1] = held[1]

    remote(held.at[1 - c], attn.at[1 - c], swap_send, swap_recv, at(z, y, 1 - c)).wait_recv()
    for i in range(4, 8):
        load(i).wait()

    CH = COLUMNS
    NC = 4096 // CH
    chip = z * 4 + y
    rows_of = lambda who: pl.ds(pl.multiple_of(who * 32, 32), 32)

    def sent(n, step):
        to = lax.rem(tp + step, 4)
        return remote(
            part.at[n, to], got.at[n, step], r_send.at[n, step], r_recv.at[n, step], (sp, to)
        )

    def gather(n, step):
        to = lax.rem(tp + step, 4)
        block = normed.at[n, c, rows_of(tp)]
        return remote(block, block, a_send.at[n, step], a_recv.at[n, step], (sp, to))

    def arrived(n, step):
        frm = lax.rem(tp + 4 - step, 4)
        block = normed.at[n, c, rows_of(frm)]
        return remote(block, block, a_send.at[n, step], a_recv.at[n, step], (sp, frm))

    def pair(n, step):
        block = normed.at[n, c, rows_of(lax.rem(tp + 4 - step, 4))]
        return remote(block, block, p_send.at[n, step], p_recv.at[n, step], at(z, y, 1 - c))

    def slots(src, dst, send, recv, n):
        for dz, dy in FAR_FIRST:
            zz = lax.rem(z + jnp.where(c == 0, dz, 4 - dz), 4)
            yy = lax.rem(y + jnp.where(c == 0, dy, 4 - dy), 4)
            remote(
                src.at[n, zz * 4 + yy], dst.at[n, chip], send.at[n], recv.at[n], at(zz, yy, c)
            ).start()

    def all_of(ref, sem, n):
        block = ref.at[n, pl.ds(0, 15)]
        return pltpu.make_async_copy(block, block, sem.at[n])

    for t in range(1, 8):
        code(t).wait_recv()

    def chip_line(ref):
        return jnp.concatenate(
            [ref[h * 4] + ref[h * 4 + 1] + ref[h * 4 + 2] + ref[h * 4 + 3] for h in range(2)], axis=1
        )

    table = chip_line(codes)
    slot = lax.broadcasted_iota(jnp.int32, (256, 256), 0)
    token = lax.broadcasted_iota(jnp.int32, (256, 256), 1)
    wanted = (((slot // 16) * 2 + c) * 4 + tp) * 2 + slot % 2
    wanted = jnp.where((slot // 2) % 8 == token // 32, wanted, -1).astype(jnp.float32)
    picks = jnp.zeros((256, 256), jnp.float32)
    pays = jnp.zeros((256, 256), jnp.float32)
    for k in range(4):
        same = table[k : k + 1] == wanted
        picks = picks + jnp.where(same, 1.0, 0.0)
        pays = pays + jnp.where(same, table[4 + k : 5 + k], 0.0)
    dmat[...] = picks.astype(jnp.bfloat16)
    cmat[...] = pays.T.reshape(2, 128, 256).astype(jnp.bfloat16)

    def project(n):
        cols = pl.ds(n * CH, CH)
        p = jnp.dot(attn[0], wn[:, cols], preferred_element_type=jnp.float32)
        p = p + jnp.dot(attn[1], wb[:, cols], preferred_element_type=jnp.float32)
        part[n] = p.astype(jnp.bfloat16).reshape(4, 32, CH)
        for step in range(1, 4):
            sent(n, step).start()

    squares = []

    def add_up(n):
        for step in range(1, 4):
            sent(n, step).wait_recv()
        cols = pl.ds(n * CH, CH)
        total = res[:, cols].astype(jnp.float32) + part[n, tp].astype(jnp.float32)
        for step in range(1, 4):
            total = total + got[n, step].astype(jnp.float32)
        stream[:, cols] = total
        normed[n, c, rows_of(tp)] = (total * gain[:, cols]).astype(jnp.bfloat16)
        for step in range(1, 4):
            gather(n, step).start()
        pair(n, 0).start()
        sq = total * total
        for k in range(CH // 128):
            squares.append(sq[:, k * 128 : (k + 1) * 128])

    def forward(n):
        for step in range(1, 4):
            arrived(n, step).wait_recv()
            pair(n, step).start()

    def paired(n, step):
        block = normed.at[n, 1 - c, rows_of(lax.rem(tp + 4 - step, 4))]
        return remote(block, block, p_send.at[n, step], p_recv.at[n, step], at(z, y, 1 - c))

    def dispatch(n):
        for step in range(4):
            paired(n, step).wait_recv()
        rows = normed[n].reshape(256, CH)
        picked = jnp.dot(dmat[...], rows, preferred_element_type=jnp.float32).astype(jnp.bfloat16)
        outb[n] = picked.reshape(16, 16, CH)
        slots(outb, inb, d_send, d_recv, n)
        inb[n, chip] = outb[n, chip]

    def rate(t):
        to = lax.rem(me + t, 8)
        return remote(
            scales.at[me], scales.at[me], g_send.at[t], g_recv.at[t], (z * 8 + y * 2 + to // 4, to % 4)
        )

    def take_in(n):
        all_of(inb, d_recv, n).wait()
        more = jnp.dot(
            inb[n].reshape(256, CH), wgu[n * CH : (n + 1) * CH, :], preferred_element_type=jnp.float32
        )
        gu[...] = more if n == 0 else gu[...] + more

    for i in range(8, 14):
        load(i).wait()
    project(0)
    project(1)
    for i in range(NC + 2):
        if i < NC:
            add_up(i)
        if i == NC - 1:
            mean = jnp.sum(sum(squares[1:], squares[0]), axis=1, keepdims=True) * (1.0 / 4096)
            own_rate = lax.rsqrt(mean + norm_epsilon)
            scales[me] = jnp.broadcast_to(
                jnp.sum(jnp.where(place, own_rate, 0.0), axis=0, keepdims=True), (8, 128)
            )
            for t in range(1, 8):
                rate(t).start()
        if i + 2 < NC:
            project(i + 2)
        if 0 <= i - 1 < NC:
            forward(i - 1)
        if i - 2 == NC - 1:
            for t in range(1, 8):
                rate(t).wait_recv()
            rates = chip_line(scales)[:1]
            by_slot = jnp.sum(picks * rates, axis=1, keepdims=True)
            high = by_slot.astype(jnp.bfloat16).astype(jnp.float32)
            first = lax.broadcasted_iota(jnp.int32, (256, 128), 1)
            pieces = jnp.where(first == 0, high, jnp.where(first == 1, by_slot - high, 0.0))
            rout[0] = pieces.astype(jnp.bfloat16).reshape(16, 16, 128)
            slots(rout, rin, h_send, h_recv, 0)
            rin[0, chip] = rout[0, chip]
        if 0 <= i - 2:
            dispatch(i - 2)
        if 0 <= i - 1 - BEHIND:
            take_in(i - 1 - BEHIND)

    for n in range(NC + 1 - BEHIND, NC):
        take_in(n)
    def silu_up(both):
        gate, up = both[:, :256], both[:, 256:]
        return (gate / (1.0 + jnp.exp(-gate)) * up).astype(jnp.bfloat16)

    all_of(rin, h_recv, 0).wait()
    hidden = silu_up(
        gu[...] * jnp.sum(rin[0].reshape(256, 128).astype(jnp.float32), axis=1, keepdims=True)
    )
    for n in range(NC):
        made = jnp.dot(hidden, wd[:, n * CH : (n + 1) * CH], preferred_element_type=jnp.float32)
        back[n] = made.astype(jnp.bfloat16).reshape(16, 16, CH)
        slots(back, ret, e_send, e_recv, n)
        ret[n, chip] = back[n, chip]

    lanes = lax.broadcasted_iota(jnp.int32, (128, 256), 1)
    mark_row = lanes == lax.broadcasted_iota(jnp.int32, (128, 256), 0) + c * 128
    by_token = jnp.sum(jnp.where(mark_row, rates, 0.0), axis=1, keepdims=True)

    both = jnp.dot(normed[0, c], sgu[:CH, :], preferred_element_type=jnp.float32)
    for n in range(1, NC):
        both = both + jnp.dot(
            normed[n, c], sgu[n * CH : (n + 1) * CH, :], preferred_element_type=jnp.float32
        )
    hidden = silu_up(both * by_token)
    for n in range(NC):
        mine[n] = jnp.dot(hidden, sd[:, n * CH : (n + 1) * CH], preferred_element_type=jnp.float32)

    def to_pair(n):
        return remote(theirs.at[n], from_pair.at[n], t_send.at[n], t_recv.at[n], at(z, y, 1 - c))

    def to_owner(n, step):
        to = lax.rem(tp + step, 4)
        return remote(
            part2.at[n, to], got2.at[n, step], s_send.at[n, step], s_recv.at[n, step], (sp, to)
        )

    def over(step):
        to = lax.rem(tp + step, 4)
        return remote(
            part3.at[to], got3.at[step], t3_send.at[step], t3_recv.at[step],
            (z * 8 + y * 2 + 1 - c, to),
        )

    last = NC - 1

    def finish(n):
        total = stream[:, n * CH : (n + 1) * CH] + part2[n, tp].astype(jnp.float32)
        for step in range(1, 4):
            to_owner(n, step).wait_recv()
            total = total + got2[n, step].astype(jnp.float32)
        if n == last:
            for step in range(4):
                over(step).wait_recv()
                total = total + got3[step].astype(jnp.float32)
        out_ref[:, n * CH : (n + 1) * CH] = total

    def merge(n):
        to_pair(n).wait_recv()
        both = mine[n] + from_pair[n].astype(jnp.float32)
        part2[n] = both.astype(jnp.bfloat16).reshape(4, 32, CH)
        for step in range(1, 4):
            to_owner(n, step).start()

    for i in range(NC):
        all_of(ret, e_recv, i).wait()
        rows = ret[i].reshape(256, CH)
        away = jnp.dot(cmat[1 - c], rows, preferred_element_type=jnp.float32).astype(jnp.bfloat16)
        if i < last:
            theirs[i] = away
            to_pair(i).start()
            mine[i] = mine[i] + jnp.dot(cmat[c], rows, preferred_element_type=jnp.float32)
        else:
            part3[...] = away.reshape(4, 32, CH)
            for step in (2, 1, 3, 0):
                over(step).start()
            ours = mine[i] + jnp.dot(cmat[c], rows, preferred_element_type=jnp.float32)
            part2[i] = ours.astype(jnp.bfloat16).reshape(4, 32, CH)
            for step in (2, 1, 3):
                to_owner(i, step).start()
        if 0 <= i - 1:
            merge(i - 1)
        if 0 <= i - 2:
            finish(i - 2)
    finish(last - 1)
    finish(last)

    for role in range(2):

        @pl.when(c == role)
        def _(role=role):
            q_over(1 - role).wait_send()
            kv_over(1 - role).wait_send()

    for step in range(1, 4):

        @pl.when(c == 1)
        def _(step=step):
            b1(step).wait_send()

        @pl.when(z + step < 4)
        def _(step=step):
            n1(step).wait_send()

    @pl.when(c == 0)
    def _():
        def done(t, carry):
            for step in range(1, 4):

                @pl.when((t < z) | (y + step < 4))
                def _(step=step):
                    n2(t, step).wait_send()

            return carry

        lax.fori_loop(0, z + 1, done, 0)

    @pl.when(c == 1)
    def _():
        def done(t, carry):
            for step in range(1, 4):

                @pl.when(z + step < 4)
                def _(step=step):
                    b2(t, step).wait_send()

            return carry

        lax.fori_loop(0, 4, done, 0)

    remote(held.at[1 - c], attn.at[1 - c], swap_send, swap_recv, at(z, y, 1 - c)).wait_send()
    for t in range(1, 8):
        code(t).wait_send()
    for step in range(4):
        over(step).wait_send()
    for t in range(1, 8):
        rate(t).wait_send()
    all_of(rout, h_send, 0).wait()
    for n in range(NC):
        for step in range(1, 4):
            gather(n, step).wait_send()
        for step in range(4):
            pair(n, step).wait_send()
        for step in range(1, 4):
            sent(n, step).wait_send()
            to_owner(n, step).wait_send()
        all_of(outb, d_send, n).wait()
        all_of(back, e_send, n).wait()
        if n < last:
            to_pair(n).wait_send()


def layer(*args):
    any_ = pl.BlockSpec(memory_space=pltpu.HBM)
    dma = pltpu.SemaphoreType.DMA
    f32, b16 = jnp.float32, jnp.bfloat16
    vm = pltpu.VMEM
    return pl.pallas_call(
        layer_kernel,
        out_shape=jax.ShapeDtypeStruct((32, 4096), f32),
        in_specs=[any_] * len(args),
        out_specs=pl.BlockSpec(memory_space=pltpu.VMEM),
        scratch_shapes=[
            vm((4, 4, 256, 256), b16), vm((4, 4, 256, 512), b16),
            vm((2, 128, 512), b16), vm((2, 128, 512), b16), vm((2, 128, 512), b16), vm((2, 128, 512), b16),
            vm((4, 256, 128), f32), vm((4, 256, 128), f32), vm((4, 256, 128), f32),
            vm((2, 256, 128), f32), vm((2, 256, 128), f32), vm((2, 256, 256), f32),
            vm((512, 4096), b16), vm((512, 4096), b16), vm((32, 4096), b16),
            vm((BLOCKS, 4, 32, COLUMNS), b16), vm((BLOCKS, 4, 32, COLUMNS), b16), vm((32, 4096), f32),
            vm((BLOCKS, 2, 128, COLUMNS), b16),
            vm((4, 4096), f32), vm((2, 4096), f32), vm((1, 4096), f32), vm((4, 32), jnp.int32), vm((4, 32), f32),
            vm((4096, 512), b16), vm((256, 4096), b16), vm((4096, 512), b16), vm((256, 4096), b16),
            vm((8, 8, 128), f32), vm((8, 8, 128), f32), vm((1, 16, 16, 128), b16), vm((1, 16, 16, 128), b16),
            vm((256, 256), b16), vm((2, 128, 256), b16),
            *[vm((BLOCKS, 16, 16, COLUMNS), b16)] * 4,
            vm((256, 512), f32), vm((BLOCKS, 128, COLUMNS), f32),
            vm((BLOCKS, 128, COLUMNS), b16), vm((BLOCKS, 128, COLUMNS), b16),
            vm((BLOCKS, 4, 32, COLUMNS), b16), vm((BLOCKS, 4, 32, COLUMNS), b16),
            vm((4, 32, COLUMNS), b16), vm((4, 32, COLUMNS), b16),
            dma((5,)), dma((14,)), dma((2,)),
            dma((4,)), dma((4, 2)), dma((4,)), dma((4, 2)),
            dma((4, 4)), dma((4, 4)), dma((4, 4)), dma((4, 4)),
            dma((2,)), dma(()), dma(()),
            dma((BLOCKS, 4)), dma((BLOCKS, 4)), dma((BLOCKS, 4)), dma((BLOCKS, 4)),
            dma((8,)), dma((8,)), dma((BLOCKS, 4)), dma((BLOCKS, 4)),
            dma((BLOCKS,)), dma((BLOCKS,)), dma((BLOCKS,)), dma((BLOCKS,)), dma((BLOCKS,)), dma((BLOCKS,)),
            dma((BLOCKS, 4)), dma((BLOCKS, 4)),
            dma((8,)), dma((8,)), dma((1,)), dma((1,)), dma((4,)), dma((4,)),
        ],
        compiler_params=pltpu.CompilerParams(
            collective_id=0, has_side_effects=True, vmem_limit_bytes=56 * 2**20
        ),
        name="layer",
    )(*args)


def local(
    query_narrow, key_narrow, value_narrow, gates_narrow, query_broad, key_broad, value_broad,
    gates_broad, project_narrow, project_broad, residual, norm_gain, route_ids, route_weight,
    expert_gate, expert_up, expert_down, shared_gate, shared_up, shared_down,
):
    return layer(
        query_narrow, key_narrow, value_narrow, gates_narrow.T, query_broad, key_broad, value_broad,
        gates_broad.T, project_narrow, project_broad, residual, norm_gain.reshape(1, -1), route_ids.T,
        route_weight.T, expert_gate, expert_up, expert_down, shared_gate, shared_up, shared_down,
    ).astype(jnp.bfloat16)


def solution(mesh):
    placed = (
        P("sp", "tp"),
        P("sp", "tp"),
        P("sp", "tp"),
        P(None, "tp"),
        P("sp", "tp"),
        P("sp", "tp"),
        P("sp", "tp"),
        P(None, "tp"),
        P("tp", None),
        P("tp", None),
        P("sp", None),
        P(),
        P(("sp", "tp"), None),
        P(("sp", "tp"), None),
        P(("sp", "tp"), None, None),
        P(("sp", "tp"), None, None),
        P(("sp", "tp"), None, None),
        P(None, "tp"),
        P(None, "tp"),
        P("tp", None),
    )
    return jax.shard_map(
        local, mesh=mesh, in_specs=placed, out_specs=P(("sp", "tp"), None), check_vma=False
    )
```

```python
import math

import jax
import jax.numpy as jnp
from jax import lax
from jax.experimental import pallas as pl
from jax.experimental.pallas import tpu as pltpu
from jax.sharding import PartitionSpec as P

norm_epsilon = 1e-06
COLUMNS = 512
BLOCKS = 4096 // COLUMNS
BEHIND = 6
FAR_FIRST = (
    (2, 2), (1, 2), (2, 3), (3, 2), (2, 1), (1, 1), (1, 3), (3, 3), (3, 1),
    (2, 0), (0, 2), (1, 0), (0, 1), (3, 0), (0, 3),
)

MESH = pl.DeviceIdType.MESH
LOG2E = math.log2(math.e)


def flash_heads(q_ref, kv, gate_rows, m_ref, l_ref, acc_ref, heads, size, diagonal):
    keys = kv[:, :size]
    values = kv[:, size:]
    rows = q_ref.shape[0] * q_ref.shape[1]
    length = keys.shape[0]
    scale = size ** (-0.5) * LOG2E
    for h in range(heads):
        q = q_ref[:, :, h * size : (h + 1) * size].reshape(rows, size)
        s = lax.dot_general(q, keys, (((1,), (1,)), ((), ())), preferred_element_type=jnp.float32)
        s = s * scale - gate_rows[h : h + 1, :]
        if diagonal:
            at = lax.broadcasted_iota(jnp.int32, (rows, length), 0)
            to = lax.broadcasted_iota(jnp.int32, (rows, length), 1)
            s = jnp.where(to <= at, s, -jnp.inf)
        top = jnp.broadcast_to(jnp.max(s, axis=1, keepdims=True), (rows, 128))
        if not diagonal:
            before = m_ref[h]
            top = jnp.maximum(before, top)
        p = jnp.exp2(s - jnp.concatenate([top] * (length // 128), axis=1))
        total = jnp.broadcast_to(jnp.sum(p, axis=1, keepdims=True), (rows, 128))
        out = jnp.dot(p.astype(jnp.bfloat16), values, preferred_element_type=jnp.float32)
        if not diagonal:
            factor = jnp.exp2(before - top)
            total = total + l_ref[h] * factor
            out = out + acc_ref[h] * jnp.concatenate([factor] * (size // 128), axis=1)
        m_ref[h] = top
        l_ref[h] = total
        acc_ref[h] = out


def layer_kernel(
    qn_in, kn_in, vn_in, gn_in, qb_in, kb_in, vb_in, gb_in, pn_in, pb_in, res_in, gain_in,
    ids_in, rw_in, eg_in, eu_in, ed_in, sg_in, su_in, sd_in,
    out_ref,
    nkv, bkv, qn, qb, attn, held, mn, ln, accn, mb, lb, accb, wn, wb, res, part, got, stream, normed,
    gn, gb, gain, ids, rw, wgu, wd, sgu, sd, codes, scales, rout, rin, dmat, cmat, outb, inb, back, ret, gu, mine,
    theirs, from_pair, part2, got2, part3, got3,
    own_sem, load_sem, own_send, n1_send, n1_recv, b1_send, b1_recv, n2_send, n2_recv, b2_send,
    b2_recv, q_recv, swap_send, swap_recv, r_send, r_recv, a_send, a_recv,
    c_send, c_recv, p_send, p_recv, d_send, d_recv, e_send, e_recv, t_send, t_recv, s_send, s_recv,
    g_send, g_recv, h_send, h_recv, t3_send, t3_recv,
):
    sp = lax.axis_index("sp")
    tp = lax.axis_index("tp")
    z = sp // 8
    y = (sp // 2) % 4
    c = sp % 2
    half = pl.ds(pl.multiple_of(c * 128, 128), 128)

    def at(zz, yy, cc):
        return (zz * 8 + yy * 2 + cc, tp)

    barrier = pltpu.get_barrier_semaphore()

    def greet(to):
        pl.semaphore_signal(barrier, inc=1, device_id=to, device_id_type=MESH)

    def greet_chip(t, carry):
        greet(at(lax.rem(z + t // 4, 4), lax.rem(y + t % 4, 4), c))
        return carry

    lax.fori_loop(1, 16, greet_chip, 0)
    for step in range(1, 4):
        greet(at(lax.rem(z + step, 4), y, 1 - c))
        greet(at(z, lax.rem(y + step, 4), 1 - c))
        for cc in range(2):
            greet((z * 8 + y * 2 + cc, lax.rem(tp + step, 4)))
    greet(at(z, y, 1 - c))

    loads = [
        (gn_in, gn), (gb_in, gb), (ids_in, ids), (rw_in, rw), (gain_in, gain),
        (res_in.at[pl.ds(pl.multiple_of(tp * 32, 32), 32)], res),
        (pn_in, wn), (pb_in, wb),
        (sg_in, sgu.at[:, pl.ds(0, 256)]), (su_in, sgu.at[:, pl.ds(256, 256)]), (sd_in, sd),
        (eg_in.at[0], wgu.at[:, pl.ds(0, 256)]), (eu_in.at[0], wgu.at[:, pl.ds(256, 256)]),
        (ed_in.at[0], wd),
    ]

    def load(i):
        return pltpu.make_async_copy(loads[i][0], loads[i][1], load_sem.at[i])

    for i in range(6):
        load(i).start()
    pl.semaphore_wait(barrier, 28)

    def remote(src, dst, send, recv, to):
        return pltpu.make_async_remote_copy(
            src_ref=src, dst_ref=dst, send_sem=send, recv_sem=recv, device_id=to, device_id_type=MESH
        )

    own_n = nkv.at[z, y, half]
    own_b = bkv.at[z, y, half]
    owns = (
        (kn_in, nkv.at[z, y, half, pl.ds(0, 128)]), (vn_in, nkv.at[z, y, half, pl.ds(128, 128)]),
        (kb_in, bkv.at[z, y, half, pl.ds(0, 256)]), (vb_in, bkv.at[z, y, half, pl.ds(256, 256)]),
    )

    def own(i):
        return pltpu.make_async_copy(owns[i][0], owns[i][1], own_sem.at[i])

    q_sides = ((qn_in, qn), (qb_in, qb))

    def q_own(role):
        return pltpu.make_async_copy(q_sides[role][0], q_sides[role][1].at[c], own_sem.at[4])

    def q_over(role):
        return remote(
            q_sides[role][0], q_sides[role][1].at[c], own_send.at[0], q_recv.at[0], at(z, y, role)
        )

    def kv_over(role):
        block = (own_n, own_b)[role]
        return remote(block, block, own_send.at[1], q_recv.at[1], at(z, y, role))

    def n1(step):
        return remote(own_n, own_n, n1_send.at[step], n1_recv.at[z, c], at(z + step, y, 0))

    def b1(step):
        return remote(
            own_b, own_b, b1_send.at[step], b1_recv.at[y, c], at(z, lax.rem(y + step, 4), 1)
        )

    for i in range(4):
        own(i).start()
    for role in range(2):

        @pl.when(c == role)
        def _(role=role):
            q_own(role).start()
            q_over(1 - role).start()

    for i in range(4):
        own(i).wait()
    for step, onward in ((1, 3), (3, 2), (2, 1)):
        b1(step).start()

        @pl.when(z + onward < 4)
        def _(onward=onward):
            n1(onward).start()

    for role in range(2):

        @pl.when(c == role)
        def _(role=role):
            kv_over(1 - role).start()

    me = c * 4 + tp
    for i in range(4):
        load(i).wait()
    lane = lax.broadcasted_iota(jnp.int32, (8, 128), 1)
    row = lax.broadcasted_iota(jnp.int32, (32, 128), 0)
    place = lax.broadcasted_iota(jnp.int32, (32, 128), 1) == row + tp * 32
    spot = place.astype(jnp.bfloat16)
    put = lambda a: jnp.dot(a.astype(jnp.bfloat16), spot, preferred_element_type=jnp.float32)
    placed_ids = put(ids[...].astype(jnp.float32))
    placed_rw = put(rw[...])
    inside = (lane[:4] // 32) == tp
    key_ids = jnp.where(inside, placed_ids, -1.0)
    names = lax.broadcasted_iota(jnp.int32, (128, 128), 0).astype(jnp.float32)
    later = (
        lax.broadcasted_iota(jnp.int32, (128, 128), 0) < lax.broadcasted_iota(jnp.int32, (128, 128), 1)
    ).astype(jnp.bfloat16)
    hits = [jnp.where(key_ids[k : k + 1] == names, 1.0, 0.0) for k in range(4)]
    before = jnp.dot(
        (hits[0] + hits[1] + hits[2] + hits[3]).astype(jnp.bfloat16), later,
        preferred_element_type=jnp.float32,
    )
    for k in range(4):
        rank = jnp.sum(hits[k] * before, axis=0, keepdims=True)
        codes[me, k : k + 1] = placed_ids[k : k + 1] * 2.0 + rank
        codes[me, 4 + k : 5 + k] = placed_rw[k : k + 1]

    def code(t):
        to = lax.rem(me + t, 8)
        return remote(
            codes.at[me], codes.at[me], c_send.at[t], c_recv.at[t], (z * 8 + y * 2 + to // 4, to % 4)
        )

    for t in range(1, 8):
        code(t).start()

    def gate_rows(ref, zz, yy):
        return ref[:, pl.ds(pl.multiple_of((zz * 4 + yy) * 256, 256), 256)] * LOG2E

    def own_wait(role):
        block = (nkv, bkv)[role].at[z, y, pl.ds((1 - role) * 128, 128)]
        remote(block, block, own_send.at[1], q_recv.at[1], at(z, y, 1 - role)).wait_recv()

    def q_wait(role):
        q_own(role).wait()
        there = q_sides[role][1].at[1 - c]
        remote(there, there, own_send.at[0], q_recv.at[0], at(z, y, 1 - role)).wait_recv()

    def n2(zz, step):
        return remote(
            nkv.at[zz, y], nkv.at[zz, y], n2_send.at[zz, step], n2_recv.at[zz, y],
            at(z, lax.rem(y + step, 4), 0),
        )

    def b2(yy, step):
        return remote(
            bkv.at[z, yy], bkv.at[z, yy], b2_send.at[yy, step], b2_recv.at[z, yy],
            at(z + step, y, 1),
        )

    @pl.when(c == 0)
    def _():
        own_wait(0)
        q_wait(0)

        def send_on(zz):
            for step in range(1, 4):
                @pl.when((zz < z) | (y + step < 4))
                def _(step=step):
                    n2(zz, step).start()

        def block(zz, yy, diagonal):
            flash_heads(
                qn, nkv[zz, yy], gate_rows(gn, zz, yy), mn, ln, accn, 4, 128, diagonal
            )

        block(z, y, True)
        for step in range(1, 4):
            b1(step).wait_send()
        send_on(z)

        def column(t, carry):
            zz = z - t
            for cc in range(2):
                there = nkv.at[zz, y, pl.ds(cc * 128, 128)]
                remote(there, there, n1_send.at[1], n1_recv.at[zz, cc], at(zz, y, 0)).wait_recv()
            send_on(zz)
            return carry

        lax.fori_loop(1, z + 1, column, 0)
        for i in range(6, 14):
            load(i).start()

        def column_block(t, carry):
            block(z - t, y, False)
            return carry

        lax.fori_loop(1, z + 1, column_block, 0)

        def rest(t, carry):
            zz = z - t // 3
            yy = lax.rem(y + t % 3 + 1, 4)

            @pl.when((zz < z) | (yy < y))
            def _():
                remote(
                    nkv.at[zz, yy], nkv.at[zz, yy], n2_send.at[zz, 1], n2_recv.at[zz, yy],
                    at(z, yy, 0),
                ).wait_recv()
                block(zz, yy, False)

            return carry

        lax.fori_loop(0, 3 * (z + 1), rest, 0)
        for h in range(4):
            out = (accn[h] / ln[h]).astype(jnp.bfloat16)
            held[:, :, h * 128 : (h + 1) * 128] = out.reshape(2, 128, 128)
        remote(
            held.at[1], attn.at[0], swap_send, swap_recv, at(z, y, 1)
        ).start()
        attn[0] = held[0]

    @pl.when(c == 1)
    def _():
        own_wait(1)

        def send_on(yy):
            for step in (3, 2, 1):
                @pl.when(z + step < 4)
                def _(step=step):
                    b2(yy, step).start()

        def block(zz, yy, diagonal):
            flash_heads(qb, bkv[zz, yy], gate_rows(gb, zz, yy), mb, lb, accb, 2, 256, diagonal)

        send_on(y)
        q_wait(1)
        block(z, y, True)

        def turn(t):
            return lax.rem(y + jnp.where(t == 2, 3, jnp.where(t == 3, 2, t)), 4)

        def row(t, carry):
            yy = turn(t)
            for cc in range(2):
                there = bkv.at[z, yy, pl.ds(cc * 128, 128)]
                remote(there, there, b1_send.at[1], b1_recv.at[yy, cc], at(z, yy, 1)).wait_recv()
            send_on(yy)
            return carry

        lax.fori_loop(1, 4, row, 0)
        for i in range(6, 14):
            load(i).start()

        def row_block(t, carry):
            block(z, t, False)
            return carry

        lax.fori_loop(0, y, row_block, 0)

        def rest(t, carry):
            yy = turn(t)

            def one(k, inner):
                zz = z - k
                remote(
                    bkv.at[zz, yy], bkv.at[zz, yy], b2_send.at[yy, 1], b2_recv.at[zz, yy],
                    at(zz, y, 1),
                ).wait_recv()
                block(zz, yy, False)
                return inner

            return lax.fori_loop(1, z + 1, one, carry)

        lax.fori_loop(0, 4, rest, 0)
        for h in range(2):
            out = (accb[h] / jnp.concatenate([lb[h]] * 2, axis=1)).astype(jnp.bfloat16)
            held[:, :, h * 256 : (h + 1) * 256] = out.reshape(2, 128, 256)
        remote(
            held.at[0], attn.at[1], swap_send, swap_recv, at(z, y, 0)
        ).start()
        attn[1] = held[1]

    remote(held.at[1 - c], attn.at[1 - c], swap_send, swap_recv, at(z, y, 1 - c)).wait_recv()
    for i in range(4, 8):
        load(i).wait()

    CH = COLUMNS
    NC = 4096 // CH
    chip = z * 4 + y
    rows_of = lambda who: pl.ds(pl.multiple_of(who * 32, 32), 32)

    def sent(n, step):
        to = lax.rem(tp + step, 4)
        return remote(
            part.at[n, to], got.at[n, step], r_send.at[n, step], r_recv.at[n, step], (sp, to)
        )

    def gather(n, step):
        to = lax.rem(tp + step, 4)
        block = normed.at[n, c, rows_of(tp)]
        return remote(block, block, a_send.at[n, step], a_recv.at[n, step], (sp, to))

    def arrived(n, step):
        frm = lax.rem(tp + 4 - step, 4)
        block = normed.at[n, c, rows_of(frm)]
        return remote(block, block, a_send.at[n, step], a_recv.at[n, step], (sp, frm))

    def pair(n, step):
        block = normed.at[n, c, rows_of(lax.rem(tp + 4 - step, 4))]
        return remote(block, block, p_send.at[n, step], p_recv.at[n, step], at(z, y, 1 - c))

    def slots(src, dst, send, recv, n):
        for dz, dy in FAR_FIRST:
            zz = lax.rem(z + jnp.where(c == 0, dz, 4 - dz), 4)
            yy = lax.rem(y + jnp.where(c == 0, dy, 4 - dy), 4)
            remote(
                src.at[n, zz * 4 + yy], dst.at[n, chip], send.at[n], recv.at[n], at(zz, yy, c)
            ).start()

    def all_of(ref, sem, n):
        block = ref.at[n, pl.ds(0, 15)]
        return pltpu.make_async_copy(block, block, sem.at[n])

    for t in range(1, 8):
        code(t).wait_recv()

    def chip_line(ref):
        return jnp.concatenate(
            [ref[h * 4] + ref[h * 4 + 1] + ref[h * 4 + 2] + ref[h * 4 + 3] for h in range(2)], axis=1
        )

    table = chip_line(codes)
    slot = lax.broadcasted_iota(jnp.int32, (256, 256), 0)
    token = lax.broadcasted_iota(jnp.int32, (256, 256), 1)
    wanted = (((slot // 16) * 2 + c) * 4 + tp) * 2 + slot % 2
    wanted = jnp.where((slot // 2) % 8 == token // 32, wanted, -1).astype(jnp.float32)
    picks = jnp.zeros((256, 256), jnp.float32)
    pays = jnp.zeros((256, 256), jnp.float32)
    for k in range(4):
        same = table[k : k + 1] == wanted
        picks = picks + jnp.where(same, 1.0, 0.0)
        pays = pays + jnp.where(same, table[4 + k : 5 + k], 0.0)
    dmat[...] = picks.astype(jnp.bfloat16)
    cmat[...] = pays.T.reshape(2, 128, 256).astype(jnp.bfloat16)

    def project(n):
        cols = pl.ds(n * CH, CH)
        p = jnp.dot(attn[0], wn[:, cols], preferred_element_type=jnp.float32)
        p = p + jnp.dot(attn[1], wb[:, cols], preferred_element_type=jnp.float32)
        part[n] = p.astype(jnp.bfloat16).reshape(4, 32, CH)
        for step in range(1, 4):
            sent(n, step).start()

    squares = []

    def add_up(n):
        for step in range(1, 4):
            sent(n, step).wait_recv()
        cols = pl.ds(n * CH, CH)
        total = res[:, cols].astype(jnp.float32) + part[n, tp].astype(jnp.float32)
        for step in range(1, 4):
            total = total + got[n, step].astype(jnp.float32)
        stream[:, cols] = total
        normed[n, c, rows_of(tp)] = (total * gain[:, cols]).astype(jnp.bfloat16)
        for step in range(1, 4):
            gather(n, step).start()
        pair(n, 0).start()
        sq = total * total
        for k in range(CH // 128):
            squares.append(sq[:, k * 128 : (k + 1) * 128])

    def forward(n):
        for step in range(1, 4):
            arrived(n, step).wait_recv()
            pair(n, step).start()

    def paired(n, step):
        block = normed.at[n, 1 - c, rows_of(lax.rem(tp + 4 - step, 4))]
        return remote(block, block, p_send.at[n, step], p_recv.at[n, step], at(z, y, 1 - c))

    def dispatch(n):
        for step in range(4):
            paired(n, step).wait_recv()
        rows = normed[n].reshape(256, CH)
        picked = jnp.dot(dmat[...], rows, preferred_element_type=jnp.float32).astype(jnp.bfloat16)
        outb[n] = picked.reshape(16, 16, CH)
        slots(outb, inb, d_send, d_recv, n)
        inb[n, chip] = outb[n, chip]

    def rate(t):
        to = lax.rem(me + t, 8)
        return remote(
            scales.at[me], scales.at[me], g_send.at[t], g_recv.at[t], (z * 8 + y * 2 + to // 4, to % 4)
        )

    def take_in(n):
        all_of(inb, d_recv, n).wait()
        more = jnp.dot(
            inb[n].reshape(256, CH), wgu[n * CH : (n + 1) * CH, :], preferred_element_type=jnp.float32
        )
        gu[...] = more if n == 0 else gu[...] + more

    for i in range(8, 14):
        load(i).wait()
    project(0)
    project(1)
    for i in range(NC + 2):
        if i < NC:
            add_up(i)
        if i == NC - 1:
            mean = jnp.sum(sum(squares[1:], squares[0]), axis=1, keepdims=True) * (1.0 / 4096)
            own_rate = lax.rsqrt(mean + norm_epsilon)
            scales[me] = jnp.broadcast_to(
                jnp.sum(jnp.where(place, own_rate, 0.0), axis=0, keepdims=True), (8, 128)
            )
            for t in range(1, 8):
                rate(t).start()
        if i + 2 < NC:
            project(i + 2)
        if 0 <= i - 1 < NC:
            forward(i - 1)
        if i - 2 == NC - 1:
            for t in range(1, 8):
                rate(t).wait_recv()
            rates = chip_line(scales)[:1]
            by_slot = jnp.sum(picks * rates, axis=1, keepdims=True)
            high = by_slot.astype(jnp.bfloat16).astype(jnp.float32)
            first = lax.broadcasted_iota(jnp.int32, (256, 128), 1)
            pieces = jnp.where(first == 0, high, jnp.where(first == 1, by_slot - high, 0.0))
            rout[0] = pieces.astype(jnp.bfloat16).reshape(16, 16, 128)
            slots(rout, rin, h_send, h_recv, 0)
            rin[0, chip] = rout[0, chip]
        if 0 <= i - 2:
            dispatch(i - 2)
        if 0 <= i - 1 - BEHIND:
            take_in(i - 1 - BEHIND)

    for n in range(NC + 1 - BEHIND, NC):
        take_in(n)
    def silu_up(both):
        gate, up = both[:, :256], both[:, 256:]
        return (gate / (1.0 + jnp.exp(-gate)) * up).astype(jnp.bfloat16)

    all_of(rin, h_recv, 0).wait()
    hidden = silu_up(
        gu[...] * jnp.sum(rin[0].reshape(256, 128).astype(jnp.float32), axis=1, keepdims=True)
    )
    for n in range(NC):
        made = jnp.dot(hidden, wd[:, n * CH : (n + 1) * CH], preferred_element_type=jnp.float32)
        back[n] = made.astype(jnp.bfloat16).reshape(16, 16, CH)
        slots(back, ret, e_send, e_recv, n)
        ret[n, chip] = back[n, chip]

    lanes = lax.broadcasted_iota(jnp.int32, (128, 256), 1)
    mark_row = lanes == lax.broadcasted_iota(jnp.int32, (128, 256), 0) + c * 128
    by_token = jnp.sum(jnp.where(mark_row, rates, 0.0), axis=1, keepdims=True)

    both = jnp.dot(normed[0, c], sgu[:CH, :], preferred_element_type=jnp.float32)
    for n in range(1, NC):
        both = both + jnp.dot(
            normed[n, c], sgu[n * CH : (n + 1) * CH, :], preferred_element_type=jnp.float32
        )
    hidden = silu_up(both * by_token)
    for n in range(NC):
        mine[n] = jnp.dot(hidden, sd[:, n * CH : (n + 1) * CH], preferred_element_type=jnp.float32)

    def to_pair(n):
        return remote(theirs.at[n], from_pair.at[n], t_send.at[n], t_recv.at[n], at(z, y, 1 - c))

    def to_owner(n, step):
        to = lax.rem(tp + step, 4)
        return remote(
            part2.at[n, to], got2.at[n, step], s_send.at[n, step], s_recv.at[n, step], (sp, to)
        )

    def over(step):
        to = lax.rem(tp + step, 4)
        return remote(
            part3.at[to], got3.at[step], t3_send.at[step], t3_recv.at[step],
            (z * 8 + y * 2 + 1 - c, to),
        )

    last = NC - 1

    def finish(n):
        total = stream[:, n * CH : (n + 1) * CH] + part2[n, tp].astype(jnp.float32)
        for step in range(1, 4):
            to_owner(n, step).wait_recv()
            total = total + got2[n, step].astype(jnp.float32)
        if n == last:
            for step in range(4):
                over(step).wait_recv()
                total = total + got3[step].astype(jnp.float32)
        out_ref[:, n * CH : (n + 1) * CH] = total

    def merge(n):
        to_pair(n).wait_recv()
        both = mine[n] + from_pair[n].astype(jnp.float32)
        part2[n] = both.astype(jnp.bfloat16).reshape(4, 32, CH)
        for step in range(1, 4):
            to_owner(n, step).start()

    for i in range(NC):
        all_of(ret, e_recv, i).wait()
        rows = ret[i].reshape(256, CH)
        away = jnp.dot(cmat[1 - c], rows, preferred_element_type=jnp.float32).astype(jnp.bfloat16)
        if i < last:
            theirs[i] = away
            to_pair(i).start()
            mine[i] = mine[i] + jnp.dot(cmat[c], rows, preferred_element_type=jnp.float32)
        else:
            part3[...] = away.reshape(4, 32, CH)
            for step in (2, 1, 3, 0):
                over(step).start()
            ours = mine[i] + jnp.dot(cmat[c], rows, preferred_element_type=jnp.float32)
            part2[i] = ours.astype(jnp.bfloat16).reshape(4, 32, CH)
            for step in (2, 1, 3):
                to_owner(i, step).start()
        if 0 <= i - 1:
            merge(i - 1)
        if 0 <= i - 2:
            finish(i - 2)
    finish(last - 1)
    finish(last)

    for role in range(2):

        @pl.when(c == role)
        def _(role=role):
            q_over(1 - role).wait_send()
            kv_over(1 - role).wait_send()

    for step in range(1, 4):

        @pl.when(c == 1)
        def _(step=step):
            b1(step).wait_send()

        @pl.when(z + step < 4)
        def _(step=step):
            n1(step).wait_send()

    @pl.when(c == 0)
    def _():
        def done(t, carry):
            for step in range(1, 4):

                @pl.when((t < z) | (y + step < 4))
                def _(step=step):
                    n2(t, step).wait_send()

            return carry

        lax.fori_loop(0, z + 1, done, 0)

    @pl.when(c == 1)
    def _():
        def done(t, carry):
            for step in range(1, 4):

                @pl.when(z + step < 4)
                def _(step=step):
                    b2(t, step).wait_send()

            return carry

        lax.fori_loop(0, 4, done, 0)

    remote(held.at[1 - c], attn.at[1 - c], swap_send, swap_recv, at(z, y, 1 - c)).wait_send()
    for t in range(1, 8):
        code(t).wait_send()
    for step in range(4):
        over(step).wait_send()
    for t in range(1, 8):
        rate(t).wait_send()
    all_of(rout, h_send, 0).wait()
    for n in range(NC):
        for step in range(1, 4):
            gather(n, step).wait_send()
        for step in range(4):
            pair(n, step).wait_send()
        for step in range(1, 4):
            sent(n, step).wait_send()
            to_owner(n, step).wait_send()
        all_of(outb, d_send, n).wait()
        all_of(back, e_send, n).wait()
        if n < last:
            to_pair(n).wait_send()


def layer(*args):
    any_ = pl.BlockSpec(memory_space=pltpu.HBM)
    dma = pltpu.SemaphoreType.DMA
    f32, b16 = jnp.float32, jnp.bfloat16
    vm = pltpu.VMEM
    return pl.pallas_call(
        layer_kernel,
        out_shape=jax.ShapeDtypeStruct((32, 4096), f32),
        in_specs=[any_] * len(args),
        out_specs=pl.BlockSpec(memory_space=pltpu.VMEM),
        scratch_shapes=[
            vm((4, 4, 256, 256), b16), vm((4, 4, 256, 512), b16),
            vm((2, 128, 512), b16), vm((2, 128, 512), b16), vm((2, 128, 512), b16), vm((2, 128, 512), b16),
            vm((4, 256, 128), f32), vm((4, 256, 128), f32), vm((4, 256, 128), f32),
            vm((2, 256, 128), f32), vm((2, 256, 128), f32), vm((2, 256, 256), f32),
            vm((512, 4096), b16), vm((512, 4096), b16), vm((32, 4096), b16),
            vm((BLOCKS, 4, 32, COLUMNS), b16), vm((BLOCKS, 4, 32, COLUMNS), b16), vm((32, 4096), f32),
            vm((BLOCKS, 2, 128, COLUMNS), b16),
            vm((4, 4096), f32), vm((2, 4096), f32), vm((1, 4096), f32), vm((4, 32), jnp.int32), vm((4, 32), f32),
            vm((4096, 512), b16), vm((256, 4096), b16), vm((4096, 512), b16), vm((256, 4096), b16),
            vm((8, 8, 128), f32), vm((8, 8, 128), f32), vm((1, 16, 16, 128), b16), vm((1, 16, 16, 128), b16),
            vm((256, 256), b16), vm((2, 128, 256), b16),
            *[vm((BLOCKS, 16, 16, COLUMNS), b16)] * 4,
            vm((256, 512), f32), vm((BLOCKS, 128, COLUMNS), f32),
            vm((BLOCKS, 128, COLUMNS), b16), vm((BLOCKS, 128, COLUMNS), b16),
            vm((BLOCKS, 4, 32, COLUMNS), b16), vm((BLOCKS, 4, 32, COLUMNS), b16),
            vm((4, 32, COLUMNS), b16), vm((4, 32, COLUMNS), b16),
            dma((5,)), dma((14,)), dma((2,)),
            dma((4,)), dma((4, 2)), dma((4,)), dma((4, 2)),
            dma((4, 4)), dma((4, 4)), dma((4, 4)), dma((4, 4)),
            dma((2,)), dma(()), dma(()),
            dma((BLOCKS, 4)), dma((BLOCKS, 4)), dma((BLOCKS, 4)), dma((BLOCKS, 4)),
            dma((8,)), dma((8,)), dma((BLOCKS, 4)), dma((BLOCKS, 4)),
            dma((BLOCKS,)), dma((BLOCKS,)), dma((BLOCKS,)), dma((BLOCKS,)), dma((BLOCKS,)), dma((BLOCKS,)),
            dma((BLOCKS, 4)), dma((BLOCKS, 4)),
            dma((8,)), dma((8,)), dma((1,)), dma((1,)), dma((4,)), dma((4,)),
        ],
        compiler_params=pltpu.CompilerParams(
            collective_id=0, has_side_effects=True, vmem_limit_bytes=56 * 2**20
        ),
        name="layer",
    )(*args)


def local(
    query_narrow, key_narrow, value_narrow, gates_narrow, query_broad, key_broad, value_broad,
    gates_broad, project_narrow, project_broad, residual, norm_gain, route_ids, route_weight,
    expert_gate, expert_up, expert_down, shared_gate, shared_up, shared_down,
):
    return layer(
        query_narrow, key_narrow, value_narrow, gates_narrow.T, query_broad, key_broad, value_broad,
        gates_broad.T, project_narrow, project_broad, residual, norm_gain.reshape(1, -1), route_ids.T,
        route_weight.T, expert_gate, expert_up, expert_down, shared_gate, shared_up, shared_down,
    ).astype(jnp.bfloat16)


def solution(mesh):
    placed = (
        P("sp", "tp"),
        P("sp", "tp"),
        P("sp", "tp"),
        P(None, "tp"),
        P("sp", "tp"),
        P("sp", "tp"),
        P("sp", "tp"),
        P(None, "tp"),
        P("tp", None),
        P("tp", None),
        P("sp", None),
        P(),
        P(("sp", "tp"), None),
        P(("sp", "tp"), None),
        P(("sp", "tp"), None, None),
        P(("sp", "tp"), None, None),
        P(("sp", "tp"), None, None),
        P(None, "tp"),
        P(None, "tp"),
        P("tp", None),
    )
    return jax.shard_map(
        local, mesh=mesh, in_specs=placed, out_specs=P(("sp", "tp"), None), check_vma=False
    )
```
